32 devices in a mesh: sp: 16 (over z, y, x), tp: 2 (over core).
Axes of the slice: x: 2, y: 2, z: 4, core: 2. Of those that a mesh axis runs over, the one named last changes fastest.
Arguments:
- wide_inputs: bfloat16 [2048, 512], P('sp', 'tp'), may hold values from -6 to 6
- narrow_inputs: bfloat16 [2048, 512], P('sp', 'tp'), may hold values from -6 to 6
- wide_poles: float32 [2, 2, 32, 64], P(None, None, 'tp'), may hold values from -3.1416 to 3.1416, as said below
- narrow_poles: float32 [2, 2, 32, 32], P(None, None, 'tp'), may hold values from -3.1416 to 3.1416, as said below
- step_sizes: float32 [2, 2, 32], P(None, None, 'tp'), may hold values from 0 to 1, as said below
- forget: float32 [2, 2, 32, 2048], P(None, None, 'tp', 'sp'), may hold values from 0 to 2.2
- wide_in_map: float32 [2, 2, 32, 16, 64], P(None, None, 'tp'), may hold values from -2.5 to 2.5
- narrow_in_map: float32 [2, 2, 32, 16, 32], P(None, None, 'tp'), may hold values from -2.5 to 2.5
- wide_out_map: float32 [2, 2, 32, 16, 64], P(None, None, 'tp'), may hold values from -1.25 to 1.25
- narrow_out_map: float32 [2, 2, 32, 16, 32], P(None, None, 'tp'), may hold values from -2 to 2
- skip_weight: bfloat16 [2, 512], P(None, 'tp'), may hold values from -6 to 6
- gate_mix: bfloat16 [2, 32, 16, 16], P(None, 'tp'), may hold values from -1.5 to 1.5
- residual: bfloat16 [2048, 2048], P(('sp', 'tp')), may hold values from -6 to 6
- mixer_gain: float32 [1024], replicated, may hold values from 0.1 to 1.9
- out_proj: bfloat16 [1024, 2048], replicated, may hold values from -0.1875 to 0.1875
- ffn_gain: float32 [2048], replicated, may hold values from 0.1 to 1.9
- routes: int32 [2048, 2], P(('sp', 'tp')), may hold values from 0 to 31, all different within a row; in each aligned block of 64 rows (0 to 63, 64 to 127, ...) at most 8 rows name the same one
- route_weights: float32 [2048, 2], P(('sp', 'tp')), may hold values from 0.1 to 1
- gate_proj: bfloat16 [32, 2048, 1408], P(('sp', 'tp')), may hold values from -0.125 to 0.125
- up_proj: bfloat16 [32, 2048, 1408], P(('sp', 'tp')), may hold values from -0.125 to 0.125
- down_proj: bfloat16 [32, 1408, 2048], P(('sp', 'tp')), may hold values from -0.15625 to 0.15625
Outputs:
- layer_out: bfloat16 [2048, 2048], P(('sp', 'tp'))
The draws below stay inside these ranges and needn't reach their ends.
Inputs may be any that keep to these rules, and one draw needn't show every extreme that they name: `routes`: in each aligned block of 64 rows (the rows of one device), no expert is named by more than 8 entries, and the 2 experts of a row differ. `wide_poles`: along dimension 1, entry 0 (the real part) is negative and entry 1 (the imaginary part) is at least 0.1 in magnitude. `narrow_poles`: along dimension 1, entry 0 (the real part) is negative and entry 1 (the imaginary part) is at least 0.1 in magnitude. `step_sizes`: Positive.
All inputs are finite; a program needn't handle non-finite values.
Results may differ from the reference program's by a relative error of at most 0.014.
Values may be sent and summed in bfloat16 or wider, within the bound.
A program may use at most 192 MiB of HBM per device.

```python
import math
import jax
import jax.numpy as jnp
import numpy as np
from jax import lax

D = 2048
GROUPS = 32
CHANNELS = 16
WIDE_STATE = 64
NARROW_STATE = 32
FE = 1408
TOP = 2
TOK_DEV = 128
TOKENS = 2048
ROWS = 64
SETW = 512
EXPERTS = 32
CAP = 8


def pick_slow(key):
    chance = 0.5
    return jax.random.bernoulli(jax.random.fold_in(key, 101), chance, (2, 2, GROUPS))


def make_poles(key, which, states):
    slow = pick_slow(key)[:, which]
    keys = jax.random.split(jax.random.fold_in(key, 11 + which), 4)
    slow_rate = jnp.exp(jax.random.uniform(keys[0], (2, GROUPS, states), jnp.float32, math.log(0.05), math.log(0.5))) / TOKENS
    fast_rate = jnp.exp(jax.random.uniform(keys[1], (2, GROUPS, states), jnp.float32, math.log(0.02), math.log(0.1)))
    decay_re = -jnp.where(slow[:, :, None], slow_rate, fast_rate)
    signs = jnp.where(jax.random.bernoulli(keys[3], 0.5, (2, GROUPS, states)), 1.0, -1.0)
    decay_im = jax.random.uniform(keys[2], (2, GROUPS, states), jnp.float32, 0.1, 3.14) * signs
    return jnp.stack([decay_re, decay_im], axis=1).astype(jnp.float32)


def draw_wide_poles(key, part):
    return make_poles(key, 0, WIDE_STATE)


def draw_narrow_poles(key, part):
    return make_poles(key, 1, NARROW_STATE)


def draw_step_sizes(key, part):
    slow = pick_slow(key)
    base = jnp.exp(jax.random.uniform(jax.random.fold_in(key, 21), (2, 2, GROUPS), jnp.float32, math.log(0.5), math.log(2.0)))
    return (base * jnp.where(slow, math.sqrt(0.4 / TOKENS), 0.3)).astype(jnp.float32)


def draw_forget(key, part):
    keys = jax.random.split(jax.random.fold_in(key, 31), 3)
    blocks = TOKENS // TOK_DEV
    factor = jnp.exp(jax.random.uniform(keys[0], (2, 2, GROUPS, blocks), jnp.float32, math.log(0.1), math.log(1.0)))
    decay_speed = jnp.repeat(factor, TOK_DEV, axis=3) / TOKENS
    spots = jax.random.randint(keys[1], (2, 2, GROUPS, 3), 0, TOKENS)
    total_quantity = jax.random.uniform(keys[2], (2, 2, GROUPS, 3), jnp.float32, 0.22, 0.69)
    slot_positions = jnp.arange(TOKENS)[None, None, None, None, :] == spots[:, :, :, :, None]
    signal_segments = jnp.sum(jnp.where(slot_positions, total_quantity[:, :, :, :, None], 0.0), axis=3)
    return (decay_speed + signal_segments).astype(jnp.float32)


def block_levels(stream_key, extent, cuts, least, top_value):
    factor_of = 1.0
    for position, parts in cuts:
        heights = jax.random.uniform(jax.random.fold_in(jax.random.fold_in(stream_key, 6), position), (parts,), jnp.float32, least / len(cuts), top_value / len(cuts))
        factor_of = factor_of * jnp.repeat(jnp.exp(heights), extent[position] // parts).reshape((-1,) + (1,) * (len(extent) - 1 - position))
    return factor_of


def assign_block(stream_key, own, number, rows, number_of, top, reach, skew):
    sequence = jax.random.permutation(stream_key, number_of)
    packed, common = shares(number_of, rows * top, reach, skew, True), shares(number_of, rows * top, reach, skew, False)
    places = jnp.arange(number_of)

    def named(tallies, rotation):
        used = int((tallies > 0).sum())
        fixed = max(1, used // 4)
        shifted = fixed + (places - fixed + rotation * (used - fixed)) % max(1, number_of - fixed)
        return jnp.zeros((number_of,), jnp.int32).at[sequence[jnp.where(places < fixed, places, shifted)]].set(jnp.asarray(tallies, jnp.int32))

    tallies = jnp.where(number % 4 == 0, named(packed, number // 4), named(common, number - number // 4 - 1))
    mixed = jax.random.permutation(jax.random.fold_in(own, 3), number_of)
    donor, sink = mixed[0:number_of // 2 * 2:2], mixed[1:number_of // 2 * 2:2]
    slack = jnp.minimum(tallies[donor] - 1, reach - tallies[sink]) // 2
    slack = jnp.where((donor == sequence[0]) | (sink == sequence[0]) | (tallies[sink] == 0), 0, jnp.maximum(slack, 0))
    shifted = jax.random.randint(jax.random.fold_in(own, 4), (number_of // 2,), 0, 1 << 20) % (slack + 1)
    tallies = tallies.at[donor].add(-shifted).at[sink].add(shifted)
    labels = jnp.searchsorted(jnp.cumsum(tallies), jnp.arange(rows * top), side="right").astype(jnp.int32)
    table = labels.reshape(top, rows).T
    table = table[jax.random.permutation(jax.random.fold_in(own, 1), rows)]
    rotation = jax.random.randint(jax.random.fold_in(own, 2), (rows, 1), 0, top)
    return jnp.take_along_axis(table, (jnp.arange(top)[None, :] + rotation) % top, axis=1)


def shares(count, total, bound, lean, full):
    weights = [(1 << 20) // math.isqrt(rank ** lean) + 1 for rank in range(1, count + 1)]
    largest = bound if full else min(bound, max(-(-total // count), total * weights[0] // sum(weights)))
    least = 1 if total - largest >= count - 1 else 0
    counts, spare = [largest] + [least] * (count - 1), total - largest - least * (count - 1)
    while spare > 0:
        candidates = [i for i in range(1, count) if counts[i] < largest] or [i for i in range(1, count) if counts[i] < bound]
        pool, left = sum([weights[i] for i in candidates]), spare
        for i in candidates:
            more = min(bound - counts[i], max(1, left * weights[i] // pool), spare)
            counts[i] = counts[i] + more
            spare = spare - more
    return np.array(counts)


def normal_values(key, shape, spread, reach, cuts=(), kind=jnp.bfloat16):
    values = spread * jax.random.normal(key, shape, jnp.float32)
    if cuts:
        values = values * block_levels(key, shape, cuts, -0.22, 0.18)
    return jnp.clip(values, -reach, reach).astype(kind)


def setup_inputs(seed: int = 0) -> dict:
    key_list = jax.random.split(jax.random.key(seed), 22)
    wide_inputs = normal_values(key_list[0], (TOKENS, SETW), 1.0, 6.0, ((0, 16), (1, 2)))
    narrow_inputs = normal_values(key_list[1], (TOKENS, SETW), 1.0, 6.0, ((0, 16), (1, 2)))
    wide_poles = draw_wide_poles(jax.random.fold_in(key_list[21], 71), 0)
    narrow_poles = draw_narrow_poles(jax.random.fold_in(key_list[21], 71), 0)
    step_sizes = draw_step_sizes(jax.random.fold_in(key_list[21], 71), 0)
    forget = draw_forget(jax.random.fold_in(key_list[21], 71), 0)
    wide_in_map = normal_values(key_list[6], (2, 2, GROUPS, CHANNELS, WIDE_STATE), ((2 * CHANNELS) ** -0.5), 2.5, ((2, 2),), jnp.float32)
    narrow_in_map = normal_values(key_list[7], (2, 2, GROUPS, CHANNELS, NARROW_STATE), ((2 * CHANNELS) ** -0.5), 2.5, ((2, 2),), jnp.float32)
    wide_out_map = normal_values(key_list[8], (2, 2, GROUPS, CHANNELS, WIDE_STATE), ((2 * WIDE_STATE) ** -0.5), 1.25, ((2, 2),), jnp.float32)
    narrow_out_map = normal_values(key_list[9], (2, 2, GROUPS, CHANNELS, NARROW_STATE), ((2 * NARROW_STATE) ** -0.5), 2.0, ((2, 2),), jnp.float32)
    skip_weight = normal_values(key_list[10], (2, SETW), 1.0, 6.0, ((1, 2),))
    gate_mix = normal_values(key_list[11], (2, GROUPS, CHANNELS, CHANNELS), CHANNELS ** -0.5, 1.5, ((1, 2),))
    residual = normal_values(key_list[12], (TOKENS, D), 1.0, 6.0, ((0, 32),))
    mixer_gain = jnp.clip(1.0 + 0.18 * jax.random.normal(key_list[13], (2 * SETW,), jnp.float32), 0.1, 1.9)
    out_proj = normal_values(key_list[14], (2 * SETW, D), (2 * SETW) ** -0.5, 0.1875)
    ffn_gain = jnp.clip(1.0 + 0.18 * jax.random.normal(key_list[15], (D,), jnp.float32), 0.1, 1.9)
    routes_keys = jax.random.split(jax.random.fold_in(key_list[16], 1), TOKENS // ROWS)
    routes_turns = jax.random.permutation(jax.random.fold_in(key_list[16], 3), TOKENS // ROWS)
    routes = jax.vmap(lambda own, number: assign_block(jax.random.fold_in(key_list[16], 2), own, number, ROWS, EXPERTS, TOP, CAP, 2))(routes_keys, routes_turns).reshape((TOKENS, TOP))
    route_weights = jnp.clip(jnp.exp(math.log(1.0) - 2.3025851 * jax.random.uniform(key_list[17], (TOKENS, TOP), jnp.float32) ** block_levels(key_list[17], (TOKENS, TOP), ((0, 32),), -0.2, 0.2)), 0.1, 1.0)
    gate_proj = normal_values(key_list[18], (EXPERTS, D, FE), D ** -0.5, 0.125, ((0, 32),))
    up_proj = normal_values(key_list[19], (EXPERTS, D, FE), D ** -0.5, 0.125, ((0, 32),))
    down_proj = normal_values(key_list[20], (EXPERTS, FE, D), FE ** -0.5, 0.15625, ((0, 32),))
    return dict(wide_inputs=wide_inputs, narrow_inputs=narrow_inputs, wide_poles=wide_poles, narrow_poles=narrow_poles, step_sizes=step_sizes, forget=forget, wide_in_map=wide_in_map, narrow_in_map=narrow_in_map, wide_out_map=wide_out_map, narrow_out_map=narrow_out_map, skip_weight=skip_weight, gate_mix=gate_mix, residual=residual, mixer_gain=mixer_gain, out_proj=out_proj, ffn_gain=ffn_gain, routes=routes, route_weights=route_weights, gate_proj=gate_proj, up_proj=up_proj, down_proj=down_proj)


maximum_value = lax.Precision.HIGHEST
epsilon = 1e-06

def pair_step(first, second):
    first_ar, first_ai, first_br, first_bi = first
    second_ar, second_ai, second_br, second_bi = second
    return (second_ar * first_ar - second_ai * first_ai, second_ar * first_ai + second_ai * first_ar, second_ar * first_br - second_ai * first_bi + second_br, second_ar * first_bi + second_ai * first_br + second_bi)

def block_diagonal_in(matrix):
    groups, channels, states = matrix.shape
    identity = jnp.eye(groups, dtype=jnp.float32)
    return jnp.einsum('gcs,gh->gchs', matrix, identity).reshape(groups * channels, groups * states)

def block_diagonal_out(matrix):
    groups, channels, states = matrix.shape
    identity = jnp.eye(groups, dtype=jnp.float32)
    return jnp.einsum('gcs,gh->gshc', matrix, identity).reshape(groups * states, groups * channels)

def local_states(input_sequence, poles, step, decay, in_map, backward):
    decay_re = poles[0]
    decay_im = poles[1]
    states = decay_re.shape[1]
    growth = jnp.exp(decay_re)
    numer_re = growth * jnp.cos(decay_im) - 1.0
    numer_im = growth * jnp.sin(decay_im)
    denom = decay_re * decay_re + decay_im * decay_im
    factor_re = (numer_re * decay_re + numer_im * decay_im) / denom * step[:, None]
    factor_im = (numer_im * decay_re - numer_re * decay_im) / denom * step[:, None]
    input_real = factor_re[:, None, :] * in_map[0] - factor_im[:, None, :] * in_map[1]
    input_imaginary = factor_re[:, None, :] * in_map[1] + factor_im[:, None, :] * in_map[0]
    driven_real = jnp.dot(input_sequence, block_diagonal_in(input_real), precision=maximum_value)
    driven_imaginary = jnp.dot(input_sequence, block_diagonal_in(input_imaginary), precision=maximum_value)
    flat_re = decay_re.reshape(-1)[None]
    flat_im = decay_im.reshape(-1)[None]
    magnitude = jnp.exp(flat_re - jnp.repeat(jnp.transpose(decay), states, axis=1))
    return lax.associative_scan(pair_step, (magnitude * jnp.cos(flat_im), magnitude * jnp.sin(flat_im), driven_real, driven_imaginary), reverse=backward, axis=0)

def read_out(hidden_state_real, hidden_state_imaginary, output_matrix):
    return jnp.dot(hidden_state_real, block_diagonal_out(output_matrix[0]), precision=maximum_value) - jnp.dot(hidden_state_imaginary, block_diagonal_out(output_matrix[1]), precision=maximum_value)

def finish_set(input_sequence, total, skip_row, gate_block):
    shaped = total + skip_row.astype(jnp.float32)[None] * input_sequence
    active = jax.nn.gelu(shaped, approximate=True)
    gate_full = block_diagonal_in(gate_block.astype(jnp.float32))
    opened = jax.nn.sigmoid(jnp.dot(active, gate_full, precision=maximum_value))
    return (active * opened).astype(jnp.bfloat16)

def run_set(inputs, poles, steps, decay, in_map, output_matrix, skip_row, gate_block):
    blocks = TOKENS // TOK_DEV
    groups = poles.shape[2]
    states = poles.shape[3]
    input_sequence = inputs.astype(jnp.float32)
    signal_blocks = input_sequence.reshape(blocks, TOK_DEV, groups * CHANNELS)
    total = jnp.zeros((TOKENS, groups * CHANNELS), jnp.float32)
    for direction in range(2):
        decay_blocks = jnp.transpose(decay[direction].reshape(groups, blocks, TOK_DEV), (1, 0, 2))
        backward = direction == 1
        edge = 0 if backward else -1

        def stepper(carry, pieces):
            piece, piece_decay = pieces
            prod_re, prod_im, hidden_state_real, hidden_state_imaginary = local_states(piece, poles[direction], steps[direction], piece_decay, in_map[direction], backward)
            full_re = hidden_state_real + prod_re * carry[0][None] - prod_im * carry[1][None]
            full_im = hidden_state_imaginary + prod_re * carry[1][None] + prod_im * carry[0][None]
            return ((full_re[edge], full_im[edge]), read_out(full_re, full_im, output_matrix[direction]))
        start = (jnp.zeros((groups * states,), jnp.float32), jnp.zeros((groups * states,), jnp.float32))
        _, outputs = lax.scan(stepper, start, (signal_blocks, decay_blocks), reverse=backward)
        total = total + outputs.reshape(TOKENS, groups * CHANNELS)
    return finish_set(input_sequence, total, skip_row, gate_block)

def reference(wide_inputs, narrow_inputs, wide_poles, narrow_poles, step_sizes, forget, wide_in_map, narrow_in_map, wide_out_map, narrow_out_map, skip_weight, gate_mix, residual, mixer_gain, out_proj, ffn_gain, routes, route_weights, gate_proj, up_proj, down_proj):
    wide_mix = run_set(wide_inputs, wide_poles, step_sizes[:, 0], forget[:, 0], wide_in_map, wide_out_map, skip_weight[0], gate_mix[0])
    narrow_mix = run_set(narrow_inputs, narrow_poles, step_sizes[:, 1], forget[:, 1], narrow_in_map, narrow_out_map, skip_weight[1], gate_mix[1])
    joined = jnp.concatenate([wide_mix, narrow_mix], axis=1).astype(jnp.float32)
    scale = lax.rsqrt(lax.optimization_barrier(jnp.mean(joined * joined, axis=1, keepdims=True)) + epsilon)
    mixed = (joined * scale * mixer_gain).astype(jnp.bfloat16)
    projected = jnp.dot(mixed, out_proj, preferred_element_type=jnp.float32)
    hidden1 = (residual.astype(jnp.float32) + projected).astype(jnp.bfloat16)
    hidden_wide = hidden1.astype(jnp.float32)
    normed = (hidden_wide * lax.rsqrt(lax.optimization_barrier(jnp.mean(hidden_wide * hidden_wide, axis=1, keepdims=True)) + epsilon) * ffn_gain).astype(jnp.bfloat16)
    share = route_weights / lax.optimization_barrier(jnp.sum(route_weights, axis=1, keepdims=True))
    blocks = TOKENS // ROWS
    picks = routes.reshape(blocks, ROWS * TOP)
    onehot = (picks[:, :, None] == jnp.arange(EXPERTS, dtype=jnp.int32)[None, None, :]).astype(jnp.int32)
    rank = lax.optimization_barrier(jnp.sum((jnp.cumsum(onehot, axis=1) - onehot) * onehot, axis=2))
    anchor = (jnp.arange(blocks, dtype=jnp.int32) * CAP)[:, None]
    place = (picks * (blocks * CAP) + anchor + rank).reshape(-1).astype(jnp.int32)
    sectioning = jnp.zeros((EXPERTS * blocks * CAP, D), jnp.bfloat16).at[place].set(jnp.repeat(normed, TOP, axis=0))

    def apply_expert(pieces):
        rows_in, gate_w, up_w, down_w = pieces
        gate_val = jnp.dot(rows_in, gate_w, preferred_element_type=jnp.float32)
        up_val = jnp.dot(rows_in, up_w, preferred_element_type=jnp.float32)
        expert_hidden = (jax.nn.silu(gate_val) * up_val).astype(jnp.bfloat16)
        return jnp.dot(expert_hidden, down_w, preferred_element_type=jnp.float32).astype(jnp.bfloat16)
    served = lax.map(apply_expert, (sectioning.reshape(EXPERTS, blocks * CAP, D), gate_proj, up_proj, down_proj))
    taken = jnp.take(served.reshape(-1, D), place, axis=0).reshape(TOKENS, TOP, D).astype(jnp.float32)
    result = hidden1.astype(jnp.float32) + lax.optimization_barrier(jnp.sum(share[:, :, None] * taken, axis=1))
    return result.astype(jnp.bfloat16)
```

```python
import jax
import jax.numpy as jnp
from jax import lax
from jax.experimental import pallas as pl
from jax.experimental.pallas import tpu as pltpu
from jax.sharding import PartitionSpec as P

epsilon = 1e-06
SUBLANES = 8
LANES = 128


def complex_power(re, im, exponent):
    out_re, out_im = None, None
    while exponent:
        if exponent & 1:
            if out_re is None:
                out_re, out_im = re, im
            else:
                out_re, out_im = out_re * re - out_im * im, out_re * im + out_im * re
        re, im = re * re - im * im, 2.0 * re * im
        exponent >>= 1
    return out_re, out_im


def pack_list(channels, groups, sets):
    per = LANES // channels
    packs, column = [], 0
    for which, states in enumerate(sets):
        for pack in range(groups // per):
            packs.append((which, pack, column, per * states, states))
            column += per * states
    return packs, column


def order(count, direction):
    return range(count) if direction == 0 else range(count - 1, -1, -1)


def widen(rows, copies):
    return jnp.concatenate([rows] * copies, axis=1)


def block_diagonal(rows, channels, states):
    copies = LANES // channels
    tiled = widen(rows, copies)
    row = lax.broadcasted_iota(jnp.int32, tiled.shape, 0) // channels
    column = lax.broadcasted_iota(jnp.int32, tiled.shape, 1) // states
    return jnp.where(row == column, tiled, 0.0).astype(jnp.bfloat16)


def flat_row(rows, states):
    copies = rows.shape[0]
    tiled = widen(rows, copies)
    row = lax.broadcasted_iota(jnp.int32, tiled.shape, 0)
    column = lax.broadcasted_iota(jnp.int32, tiled.shape, 1) // states
    return jnp.sum(jnp.where(row == column, tiled, 0.0), axis=0, keepdims=True)


def split3(value):
    high = value.astype(jnp.bfloat16)
    rest = value - high.astype(jnp.float32)
    mid = rest.astype(jnp.bfloat16)
    low = (rest - mid.astype(jnp.float32)).astype(jnp.bfloat16)
    return high, mid, low


def owners(pack, groups, count, channels):
    which, number, _, width, states = pack
    first = which * groups + number * (LANES // channels)
    row = lax.broadcasted_iota(jnp.int32, (3 * count, width), 0) % count
    column = first + lax.broadcasted_iota(jnp.int32, (3 * count, width), 1) // states
    return jnp.where(row == column, 1.0, 0.0).astype(jnp.bfloat16)


def mixer_kernel(
    wide_u, narrow_u, wide_poles, narrow_poles, step_ref, forget_ref, wide_in, narrow_in,
    wide_out, narrow_out, skip_ref, gate_ref, out_ref,
    signal, push, keep, ends_ref, sub_ref, all_ref, carry, mixed, send_sem, recv_sem, swap_sem,
):
    tokens, half = wide_u.shape
    groups, channels = wide_in.shape[2:4]
    sets = (wide_in.shape[4], narrow_in.shape[4])
    packs, total = pack_list(channels, groups, sets)
    per = LANES // channels
    steps = tokens // SUBLANES
    span = ends_ref.shape[2]
    count = lax.axis_size("sp")
    n_tp = lax.axis_size("tp")
    mine = lax.axis_index("sp")
    tp = lax.axis_index("tp")
    barrier = pltpu.get_barrier_semaphore()
    for k in range(1, count):
        pl.semaphore_signal(
            barrier, inc=1, device_id={"sp": lax.rem(mine + k, count)},
            device_id_type=pl.DeviceIdType.MESH,
        )
    for k in range(1, n_tp):
        pl.semaphore_signal(
            barrier, inc=1, device_id={"tp": lax.rem(tp + k, n_tp)},
            device_id_type=pl.DeviceIdType.MESH,
        )

    row = lax.broadcasted_iota(jnp.int32, (tokens, tokens), 0)
    column = lax.broadcasted_iota(jnp.int32, (tokens, tokens), 1)
    weave = jnp.where(
        column == (row % SUBLANES) * steps + row // SUBLANES, 1.0, 0.0
    ).astype(jnp.bfloat16)
    unweave = jnp.where(
        row == (column % SUBLANES) * steps + column // SUBLANES, 1.0, 0.0
    ).astype(jnp.bfloat16)
    inputs = (wide_u, narrow_u)
    for which in range(2):
        signal[:, which * half : (which + 1) * half] = jnp.dot(
            weave, inputs[which][...], preferred_element_type=jnp.float32
        ).astype(jnp.bfloat16)
    held = []
    n_groups = 2 * groups
    for direction in range(2):
        rows = jnp.concatenate([forget_ref[direction, 0], forget_ref[direction, 1]], axis=0)
        pieces = jnp.concatenate(split3(jnp.exp(-rows)), axis=0)
        held.append(
            lax.dot_general(
                weave, pieces, (((1,), (1,)), ((), ())), preferred_element_type=jnp.float32
            ).astype(jnp.bfloat16)
        )
        sums = lax.dot_general(
            jnp.ones((SUBLANES, tokens), jnp.float32), rows, (((1,), (1,)), ((), ())),
            precision=lax.Precision.HIGHEST, preferred_element_type=jnp.float32,
        )
        ends_ref[direction, 6:8, :] = jnp.zeros((2, span), jnp.float32)
        ends_ref[direction, 6:7, :n_groups] = jnp.exp(-sums[:1])

    def put(direction, part, column, value):
        done = 0
        while done < value.shape[1]:
            at = column + done
            line, start = at // span, at % span
            size = min(value.shape[1] - done, span - start)
            ends_ref[direction, 3 * part + line : 3 * part + line + 1, start : start + size] = (
                value[:, done : done + size]
            )
            done += size

    eye_row = lax.broadcasted_iota(jnp.int32, (per, groups), 0)
    eye_column = lax.broadcasted_iota(jnp.int32, (per, groups), 1)
    poles, in_maps = (wide_poles, narrow_poles), (wide_in, narrow_in)
    rates = {}
    for pack in packs:
        which, number, column, width, states = pack
        cols = slice(column, column + width)
        at = slice(number * per, (number + 1) * per)
        lanes = slice(which * half + number * LANES, which * half + (number + 1) * LANES)
        owner = owners(pack, groups, n_groups, channels)
        for direction in range(2):
            re, im = poles[which][direction, 0, at, :], poles[which][direction, 1, at, :]
            growth = jnp.exp(re)
            rate_re, rate_im = growth * jnp.cos(im), growth * jnp.sin(im)
            numer = rate_re - 1.0
            step = jnp.sum(
                jnp.where(
                    eye_column == eye_row + number * per,
                    step_ref[direction, which : which + 1, :], 0.0,
                ),
                axis=1, keepdims=True,
            )
            scale = step / (re * re + im * im)
            factor_re = ((numer * re + rate_im * im) * scale)[:, None, :]
            factor_im = ((rate_im * re - numer * im) * scale)[:, None, :]
            in_re, in_im = in_maps[which][direction, 0, at], in_maps[which][direction, 1, at]
            enter = (factor_re * in_re - factor_im * in_im, factor_re * in_im + factor_im * in_re)
            for part in range(2):
                push[direction, part, :, cols] = jnp.dot(
                    signal[:, lanes],
                    block_diagonal(enter[part].reshape(LANES, states), channels, states),
                    preferred_element_type=jnp.float32,
                )
            keep[direction, :, cols] = jnp.dot(
                held[direction], owner, preferred_element_type=jnp.float32
            )
            rate_re, rate_im = flat_row(rate_re, states), flat_row(rate_im, states)
            rates[direction, column] = (rate_re, rate_im)
            h_re = jnp.zeros((SUBLANES, width), jnp.float32)
            h_im = jnp.zeros((SUBLANES, width), jnp.float32)
            kept = jnp.ones((SUBLANES, width), jnp.float32)
            for step in order(steps, direction):
                rows = slice(step * SUBLANES, (step + 1) * SUBLANES)
                hold = keep[direction, rows, cols]
                new_re = hold * (rate_re * h_re - rate_im * h_im) + push[direction, 0, rows, cols]
                h_im = hold * (rate_re * h_im + rate_im * h_re) + push[direction, 1, rows, cols]
                h_re = new_re
                kept = kept * hold
            power_re, power_im = complex_power(rate_re, rate_im, steps)
            decay_re, decay_im = kept * power_re, kept * power_im
            for part, value in enumerate((h_re, h_im, decay_re, decay_im)):
                sub_ref[direction, part, :, cols] = value
            e_re = jnp.zeros((1, width), jnp.float32)
            e_im = jnp.zeros((1, width), jnp.float32)
            for j in order(SUBLANES, direction):
                d_re, d_im = decay_re[j : j + 1], decay_im[j : j + 1]
                e_re, e_im = (
                    d_re * e_re - d_im * e_im + h_re[j : j + 1],
                    d_re * e_im + d_im * e_re + h_im[j : j + 1],
                )
            put(direction, 0, column, e_re)
            put(direction, 1, column, e_im)

    pl.semaphore_wait(barrier, count - 1 + n_tp - 1)
    copies = []
    for k in range(1, count):
        copy = pltpu.make_async_remote_copy(
            src_ref=ends_ref.at[(mine + k) // count],
            dst_ref=all_ref.at[mine],
            send_sem=send_sem.at[k],
            recv_sem=recv_sem.at[k],
            device_id={"sp": lax.rem(mine + k, count)},
            device_id_type=pl.DeviceIdType.MESH,
        )
        copy.start()
        copies.append(copy)
    all_ref[mine] = jnp.zeros(ends_ref.shape[1:], jnp.float32)
    for copy in copies:
        copy.wait()

    shares = jnp.concatenate(
        [all_ref[b, 6:7, :n_groups] for b in range(count)], axis=0
    )
    shares = jnp.concatenate(split3(shares), axis=1)
    for pack in packs:
        which, number, column, width, states = pack
        cols = slice(column, column + width)
        line, start = column // span, column % span
        kept = jnp.dot(
            shares, owners(pack, groups, n_groups, channels), preferred_element_type=jnp.float32
        )
        for direction in range(2):
            rate_re, rate_im = rates[direction, column]
            power_re, power_im = complex_power(rate_re, rate_im, tokens)
            c_re = jnp.zeros((1, width), jnp.float32)
            c_im = jnp.zeros((1, width), jnp.float32)
            for b in order(count, direction):
                use = b < mine if direction == 0 else b > mine
                e_re = all_ref[b, line : line + 1, start : start + width]
                e_im = all_ref[b, 3 + line : 4 + line, start : start + width]
                d_re, d_im = kept[b : b + 1] * power_re, kept[b : b + 1] * power_im
                c_re, c_im = (
                    jnp.where(use, d_re * c_re - d_im * c_im + e_re, c_re),
                    jnp.where(use, d_re * c_im + d_im * c_re + e_im, c_im),
                )
            for j in order(SUBLANES, direction):
                carry[direction, 0, j : j + 1, cols] = c_re
                carry[direction, 1, j : j + 1, cols] = c_im
                d_re = sub_ref[direction, 2, j : j + 1, cols]
                d_im = sub_ref[direction, 3, j : j + 1, cols]
                c_re, c_im = (
                    d_re * c_re - d_im * c_im + sub_ref[direction, 0, j : j + 1, cols],
                    d_re * c_im + d_im * c_re + sub_ref[direction, 1, j : j + 1, cols],
                )
    out_maps = (wide_out, narrow_out)
    for pack in packs:
        which, number, column, width, states = pack
        cols = slice(column, column + width)
        at = slice(number * per, (number + 1) * per)
        lanes = slice(which * half + number * LANES, which * half + (number + 1) * LANES)
        local = slice(number * LANES, (number + 1) * LANES)
        read = None
        for direction in range(2):
            rate_re, rate_im = rates[direction, column]
            h_re = carry[direction, 0, :, cols]
            h_im = carry[direction, 1, :, cols]
            for step in order(steps, direction):
                rows = slice(step * SUBLANES, (step + 1) * SUBLANES)
                hold = keep[direction, rows, cols]
                new_re = hold * (rate_re * h_re - rate_im * h_im) + push[direction, 0, rows, cols]
                h_im = hold * (rate_re * h_im + rate_im * h_re) + push[direction, 1, rows, cols]
                h_re = new_re
                push[direction, 0, rows, cols] = h_re
                push[direction, 1, rows, cols] = h_im
            for part in range(2):
                rows = out_maps[which][direction, part, at].reshape(LANES, states)
                if part:
                    rows = -rows
                term = lax.dot_general(
                    push[direction, part, :, cols].astype(jnp.bfloat16),
                    block_diagonal(rows, channels, states),
                    (((1,), (1,)), ((), ())),
                    preferred_element_type=jnp.float32,
                )
                read = term if read is None else read + term
        shaped = read + skip_ref[which : which + 1, local].astype(jnp.float32) * signal[
            :, lanes
        ].astype(jnp.float32)
        active = jax.nn.gelu(shaped, approximate=True)
        gate = block_diagonal(
            gate_ref[which, at].astype(jnp.float32).reshape(LANES, channels), channels, channels
        )
        opened = jax.nn.sigmoid(
            jnp.dot(active.astype(jnp.bfloat16), gate, preferred_element_type=jnp.float32)
        )
        mixed[:, lanes] = jnp.dot(
            unweave, (active * opened).astype(jnp.bfloat16), preferred_element_type=jnp.float32
        ).astype(jnp.bfloat16)
    rows = tokens // n_tp
    swaps = []
    for k in range(1, n_tp):
        other = lax.rem(tp + k, n_tp)
        copy = pltpu.make_async_remote_copy(
            src_ref=mixed.at[pl.ds(pl.multiple_of(other * rows, rows), rows)],
            dst_ref=out_ref.at[tp],
            send_sem=swap_sem.at[0, k],
            recv_sem=swap_sem.at[1, k],
            device_id={"tp": other},
            device_id_type=pl.DeviceIdType.MESH,
        )
        copy.start()
        swaps.append(copy)
    out_ref[tp] = mixed[pl.ds(pl.multiple_of(tp * rows, rows), rows), :]
    for copy in swaps:
        copy.wait()


def mixer(*args):
    tokens, half = args[0].shape
    groups, channels, wide_state = args[6].shape[2:]
    narrow_state = args[7].shape[4]
    _, total = pack_list(channels, groups, (wide_state, narrow_state))
    count, n_tp = lax.axis_size("sp"), lax.axis_size("tp")
    span = total // 3
    vmem = pl.BlockSpec(memory_space=pltpu.VMEM)
    return pl.pallas_call(
        mixer_kernel,
        out_shape=jax.ShapeDtypeStruct((n_tp, tokens // n_tp, 2 * half), jnp.bfloat16),
        in_specs=[vmem] * len(args),
        out_specs=vmem,
        scratch_shapes=[
            pltpu.VMEM((tokens, 2 * half), jnp.bfloat16),
            pltpu.VMEM((2, 2, tokens, total), jnp.float32),
            pltpu.VMEM((2, tokens, total), jnp.float32),
            pltpu.VMEM((2, 8, span), jnp.float32),
            pltpu.VMEM((2, 4, SUBLANES, total), jnp.float32),
            pltpu.VMEM((count, 8, span), jnp.float32),
            pltpu.VMEM((2, 2, SUBLANES, total), jnp.float32),
            pltpu.VMEM((tokens, 2 * half), jnp.bfloat16),
            pltpu.SemaphoreType.DMA((count,)),
            pltpu.SemaphoreType.DMA((count,)),
            pltpu.SemaphoreType.DMA((2, n_tp)),
        ],
        compiler_params=pltpu.CompilerParams(
            collective_id=0, has_side_effects=True, vmem_limit_bytes=24 << 20
        ),
        name="mixer",
    )(*args)


def local(
    wide_inputs, narrow_inputs, wide_poles, narrow_poles, step_sizes, forget, wide_in_map,
    narrow_in_map, wide_out_map, narrow_out_map, skip_weight, gate_mix, residual, mixer_gain,
    out_proj, ffn_gain, routes, route_weights, gate_proj, up_proj, down_proj,
):
    n_sp = lax.axis_size("sp")
    n_tp = lax.axis_size("tp")
    set_out = mixer(
        wide_inputs, narrow_inputs, wide_poles, narrow_poles, step_sizes, forget, wide_in_map,
        narrow_in_map, wide_out_map, narrow_out_map, skip_weight, gate_mix,
    )
    swapped = set_out
    rows = swapped.shape[1]
    tokens = rows * n_tp
    half = set_out.shape[2] // 2
    joined = jnp.concatenate(
        [swapped[k, :, :half] for k in range(n_tp)] + [swapped[k, :, half:] for k in range(n_tp)],
        axis=1,
    ).astype(jnp.float32)
    scale = lax.rsqrt(jnp.mean(joined * joined, axis=1, keepdims=True) + epsilon)
    mixed = (joined * scale * mixer_gain).astype(jnp.bfloat16)
    projected = jnp.dot(mixed, out_proj, preferred_element_type=jnp.float32)
    hidden1 = (residual.astype(jnp.float32) + projected).astype(jnp.bfloat16)
    hidden_wide = hidden1.astype(jnp.float32)
    normed = (
        hidden_wide
        * lax.rsqrt(jnp.mean(hidden_wide * hidden_wide, axis=1, keepdims=True) + epsilon)
        * ffn_gain
    ).astype(jnp.bfloat16)

    experts = n_sp * n_tp
    capacity = 4 * tokens // (n_tp * experts)
    top_count = routes.shape[1]
    width = normed.shape[1]
    slots = experts * capacity
    picks = routes.reshape(-1)
    entries = picks.shape[0]
    onehot = (picks[:, None] == jnp.arange(experts, dtype=jnp.int32)[None, :]).astype(jnp.bfloat16)
    earlier = (
        jnp.arange(entries)[None, :] < jnp.arange(entries)[:, None]
    ).astype(jnp.bfloat16)
    before = jnp.dot(earlier, onehot, preferred_element_type=jnp.float32)
    rank = jnp.sum(before * onehot.astype(jnp.float32), axis=1).astype(jnp.int32)
    place = (picks * capacity + rank).reshape(-1, top_count)
    hit = place[:, :, None] == jnp.arange(slots, dtype=jnp.int32)[None, None, :]
    share = route_weights / jnp.sum(route_weights, axis=1, keepdims=True)
    spot = jnp.any(hit, axis=1).astype(jnp.bfloat16)
    weight = jnp.sum(jnp.where(hit, share[:, :, None], 0.0), axis=1)
    high = lax.reduce_precision(weight, 8, 7)
    weights = jnp.concatenate([high, weight - high], axis=0).astype(jnp.bfloat16)

    sectioning = lax.dot_general(
        spot, normed, (((0,), (0,)), ((), ())), preferred_element_type=jnp.float32
    ).astype(jnp.bfloat16)
    received = lax.all_to_all(
        sectioning.reshape(experts, capacity, width),
        ("sp", "tp"),
        split_axis=0,
        concat_axis=0,
        tiled=True,
    )
    flat_rows = received.reshape(-1, width)
    gate_val = jnp.dot(flat_rows, gate_proj[0], preferred_element_type=jnp.float32)
    up_val = jnp.dot(flat_rows, up_proj[0], preferred_element_type=jnp.float32)
    expert_hidden = (jax.nn.silu(gate_val) * up_val).astype(jnp.bfloat16)
    done = jnp.dot(expert_hidden, down_proj[0], preferred_element_type=jnp.float32).astype(
        jnp.bfloat16
    )
    returned = lax.all_to_all(
        done.reshape(received.shape), ("sp", "tp"), split_axis=0, concat_axis=0, tiled=True
    )
    summed = jnp.dot(weights, returned.reshape(-1, width), preferred_element_type=jnp.float32)
    own = residual.shape[0]
    return (hidden_wide + (summed[:own] + summed[own:])).astype(jnp.bfloat16)


def solution(mesh):
    return jax.shard_map(
        local,
        mesh=mesh,
        in_specs=(
            P("sp", "tp"),
            P("sp", "tp"),
            P(None, None, "tp", None),
            P(None, None, "tp", None),
            P(None, None, "tp"),
            P(None, None, "tp", "sp"),
            P(None, None, "tp", None, None),
            P(None, None, "tp", None, None),
            P(None, None, "tp", None, None),
            P(None, None, "tp", None, None),
            P(None, "tp"),
            P(None, "tp", None, None),
            P(("sp", "tp"), None),
            P(),
            P(),
            P(),
            P(("sp", "tp"), None),
            P(("sp", "tp"), None),
            P(("sp", "tp"), None, None),
            P(("sp", "tp"), None, None),
            P(("sp", "tp"), None, None),
        ),
        out_specs=P(("sp", "tp"), None),
        check_vma=False,
    )
```

```python
import jax
import jax.numpy as jnp
from jax import lax
from jax.experimental import pallas as pl
from jax.experimental.pallas import tpu as pltpu
from jax.sharding import PartitionSpec as P

epsilon = 1e-06
SUBLANES = 8
LANES = 128


def complex_power(re, im, exponent):
    out_re, out_im = None, None
    while exponent:
        if exponent & 1:
            if out_re is None:
                out_re, out_im = re, im
            else:
                out_re, out_im = out_re * re - out_im * im, out_re * im + out_im * re
        re, im = re * re - im * im, 2.0 * re * im
        exponent >>= 1
    return out_re, out_im


def pack_list(channels, groups, sets):
    per = LANES // channels
    packs, column = [], 0
    for which, states in enumerate(sets):
        for pack in range(groups // per):
            packs.append((which, pack, column, per * states, states))
            column += per * states
    return packs, column


def order(count, direction):
    return range(count) if direction == 0 else range(count - 1, -1, -1)


def widen(rows, copies):
    return jnp.concatenate([rows] * copies, axis=1)


def block_diagonal(rows, channels, states):
    copies = LANES // channels
    tiled = widen(rows, copies)
    row = lax.broadcasted_iota(jnp.int32, tiled.shape, 0) // channels
    column = lax.broadcasted_iota(jnp.int32, tiled.shape, 1) // states
    return jnp.where(row == column, tiled, 0.0).astype(jnp.bfloat16)


def flat_row(rows, states):
    copies = rows.shape[0]
    tiled = widen(rows, copies)
    row = lax.broadcasted_iota(jnp.int32, tiled.shape, 0)
    column = lax.broadcasted_iota(jnp.int32, tiled.shape, 1) // states
    return jnp.sum(jnp.where(row == column, tiled, 0.0), axis=0, keepdims=True)


def split3(value):
    high = value.astype(jnp.bfloat16)
    rest = value - high.astype(jnp.float32)
    mid = rest.astype(jnp.bfloat16)
    low = (rest - mid.astype(jnp.float32)).astype(jnp.bfloat16)
    return high, mid, low


def owners(pack, groups, count, channels):
    which, number, _, width, states = pack
    first = which * groups + number * (LANES // channels)
    row = lax.broadcasted_iota(jnp.int32, (3 * count, width), 0) % count
    column = first + lax.broadcasted_iota(jnp.int32, (3 * count, width), 1) // states
    return jnp.where(row == column, 1.0, 0.0).astype(jnp.bfloat16)


def flip(value, bits):
    bit = 1
    while bit <= bits:
        if bits & bit:
            value = value + bit - 2 * bit * ((value // bit) % 2)
        bit *= 2
    return value


def rms_scale(value, width):
    return lax.rsqrt(jnp.sum(value * value, axis=1, keepdims=True) / width + epsilon)


def tiles(width, tile, step):
    full = width // tile
    if full:

        @pl.loop(0, full)
        def _(j):
            step(pl.ds(pl.multiple_of(j * tile, tile), tile))

    if width % tile:
        step(slice(full * tile, width))


def chunks_of(devices):
    near, far = min(16, devices // 2), min(16, devices // 4)
    half = devices // 2
    return [(a, a + near) for a in range(0, half, near)] + [
        (a, a + far) for a in range(half, devices, far)
    ]


N_SMALL = 17


def layer_kernel(*refs):
    small_hbm, refs = refs[:N_SMALL], refs[N_SMALL:]
    big_hbm, refs = refs[:4], refs[4:]
    result, refs = refs[0], refs[1:]
    small, refs = refs[:N_SMALL], refs[N_SMALL:]
    big, refs = refs[:4], refs[4:]
    (
        wide_u, narrow_u, wide_poles, narrow_poles, step_ref, forget_ref, wide_in, narrow_in,
        wide_out, narrow_out, skip_ref, gate_ref, residual, mixer_gain, ffn_gain, routes,
        route_weights,
    ) = small
    gate_w, up_w, down_w, out_w = big
    (
        signal, push, keep, ends_ref, sub_ref, all_ref, carry, mixed, out_ref, send_r, recv_r,
        send_m, recv_m, send_o, recv_o, own, hidden, normed, inner,
        small_sem, big_sem, send_sem, recv_sem, swap_sem, send_sems, recv_sems,
    ) = refs
    tokens, half = wide_u.shape
    groups, channels = wide_in.shape[2:4]
    sets = (wide_in.shape[4], narrow_in.shape[4])
    packs, total = pack_list(channels, groups, sets)
    per = LANES // channels
    steps = tokens // SUBLANES
    span = ends_ref.shape[2]
    count = lax.axis_size("sp")
    n_tp = lax.axis_size("tp")
    mine = lax.axis_index("sp")
    tp = lax.axis_index("tp")
    devices, capacity, model = send_r.shape
    own_rows = residual.shape[0]
    others = [(r // n_tp, r % n_tp) for r in range(devices)]
    peers = [{"sp": flip(mine, a), "tp": flip(tp, b)} for a, b in others]
    barrier = pltpu.get_barrier_semaphore()
    for r in range(1, devices):
        pl.semaphore_signal(
            barrier, inc=1, device_id=peers[r], device_id_type=pl.DeviceIdType.MESH
        )
    stages = []
    for i in (15, 12, 0, 1, 5, 2, 3, 4, 6, 7, 16, 8, 9, 10, 11, 13, 14):
        copy = pltpu.make_async_copy(small_hbm[i], small[i], small_sem.at[i])
        copy.start()
        stages.append(copy)
    loads = []
    for i in (3, 0, 1, 2):
        source = big_hbm[i] if i == 3 else big_hbm[i].at[0]
        copy = pltpu.make_async_copy(source, big[i], big_sem.at[i])
        copy.start()
        loads.append(copy)

    def exchange(which, source, target, r):
        return pltpu.make_async_remote_copy(
            src_ref=source.at[r], dst_ref=target.at[r],
            send_sem=send_sems.at[which, r], recv_sem=recv_sems.at[which, r],
            device_id=peers[r], device_id_type=pl.DeviceIdType.MESH,
        )

    for copy in stages[:2]:
        copy.wait()
    slots = devices * capacity
    slot = lax.broadcasted_iota(jnp.int32, (own_rows, slots), 1)
    expert = (slot // capacity) ^ (mine * n_tp + tp)
    picked = [routes[:, k : k + 1] == expert for k in range(routes.shape[1])]
    chosen = picked[0]
    for each in picked[1:]:
        chosen = jnp.logical_or(chosen, each)
    chosen = jnp.where(chosen, 1.0, 0.0)
    earlier = jnp.where(
        lax.broadcasted_iota(jnp.int32, (own_rows, own_rows), 0)
        > lax.broadcasted_iota(jnp.int32, (own_rows, own_rows), 1),
        1.0, 0.0,
    ).astype(jnp.bfloat16)
    rank = jnp.dot(earlier, chosen.astype(jnp.bfloat16), preferred_element_type=jnp.float32)
    here = rank == (slot % capacity).astype(jnp.float32)
    spot = jnp.where(here, chosen, 0.0).T.astype(jnp.bfloat16)

    def sections(value):
        rows = jnp.dot(spot, value, preferred_element_type=jnp.float32)
        return rows.reshape(devices, capacity, value.shape[1]).astype(jnp.bfloat16)

    tile = min(512, model)
    for a in range(0, model, tile):
        send_r[:, :, a : a + tile] = sections(residual[:, a : a + tile])
    recv_r[0] = send_r[0]
    pl.semaphore_wait(barrier, devices - 1)
    far = list(range(devices // 2, devices))
    near = list(range(1, devices // 2))
    first = min(4, len(far))
    early = [exchange(0, send_r, recv_r, r) for r in far[:first]]
    for copy in early:
        copy.start()
    for copy in stages[2:]:
        copy.wait()

    row = lax.broadcasted_iota(jnp.int32, (tokens, tokens), 0)
    column = lax.broadcasted_iota(jnp.int32, (tokens, tokens), 1)
    weave = jnp.where(
        column == (row % SUBLANES) * steps + row // SUBLANES, 1.0, 0.0
    ).astype(jnp.bfloat16)
    unweave = jnp.where(
        row == (column % SUBLANES) * steps + column // SUBLANES, 1.0, 0.0
    ).astype(jnp.bfloat16)
    inputs = (wide_u, narrow_u)
    for which in range(2):
        signal[:, which * half : (which + 1) * half] = jnp.dot(
            weave, inputs[which][...], preferred_element_type=jnp.float32
        ).astype(jnp.bfloat16)
    held = []
    n_groups = 2 * groups
    for direction in range(2):
        rows = jnp.concatenate([forget_ref[direction, 0], forget_ref[direction, 1]], axis=0)
        pieces = jnp.concatenate(split3(jnp.exp(-rows)), axis=0)
        held.append(
            lax.dot_general(
                weave, pieces, (((1,), (1,)), ((), ())), preferred_element_type=jnp.float32
            ).astype(jnp.bfloat16)
        )
        sums = lax.dot_general(
            jnp.ones((SUBLANES, tokens), jnp.float32), rows, (((1,), (1,)), ((), ())),
            precision=lax.Precision.HIGHEST, preferred_element_type=jnp.float32,
        )
        ends_ref[direction, 6:8, :] = jnp.zeros((2, span), jnp.float32)
        ends_ref[direction, 6:7, :n_groups] = jnp.exp(-sums[:1])

    def put(direction, part, column, value):
        done = 0
        while done < value.shape[1]:
            at = column + done
            line, start = at // span, at % span
            size = min(value.shape[1] - done, span - start)
            ends_ref[direction, 3 * part + line : 3 * part + line + 1, start : start + size] = (
                value[:, done : done + size]
            )
            done += size

    eye_row = lax.broadcasted_iota(jnp.int32, (per, groups), 0)
    eye_column = lax.broadcasted_iota(jnp.int32, (per, groups), 1)
    poles, in_maps = (wide_poles, narrow_poles), (wide_in, narrow_in)
    rates = {}
    for pack in packs:
        which, number, column, width, states = pack
        cols = slice(column, column + width)
        at = slice(number * per, (number + 1) * per)
        lanes = slice(which * half + number * LANES, which * half + (number + 1) * LANES)
        owner = owners(pack, groups, n_groups, channels)
        for direction in range(2):
            re, im = poles[which][direction, 0, at, :], poles[which][direction, 1, at, :]
            growth = jnp.exp(re)
            rate_re, rate_im = growth * jnp.cos(im), growth * jnp.sin(im)
            numer = rate_re - 1.0
            step = jnp.sum(
                jnp.where(
                    eye_column == eye_row + number * per,
                    step_ref[direction, which : which + 1, :], 0.0,
                ),
                axis=1, keepdims=True,
            )
            scale = step / (re * re + im * im)
            factor_re = ((numer * re + rate_im * im) * scale)[:, None, :]
            factor_im = ((rate_im * re - numer * im) * scale)[:, None, :]
            in_re, in_im = in_maps[which][direction, 0, at], in_maps[which][direction, 1, at]
            enter = (factor_re * in_re - factor_im * in_im, factor_re * in_im + factor_im * in_re)
            for part in range(2):
                push[direction, part, :, cols] = jnp.dot(
                    signal[:, lanes],
                    block_diagonal(enter[part].reshape(LANES, states), channels, states),
                    preferred_element_type=jnp.float32,
                )
            keep[direction, :, cols] = jnp.dot(
                held[direction], owner, preferred_element_type=jnp.float32
            )
            rate_re, rate_im = flat_row(rate_re, states), flat_row(rate_im, states)
            rates[direction, column] = (rate_re, rate_im)
            h_re = jnp.zeros((SUBLANES, width), jnp.float32)
            h_im = jnp.zeros((SUBLANES, width), jnp.float32)
            kept = jnp.ones((SUBLANES, width), jnp.float32)
            for step in order(steps, direction):
                rows = slice(step * SUBLANES, (step + 1) * SUBLANES)
                hold = keep[direction, rows, cols]
                new_re = hold * (rate_re * h_re - rate_im * h_im) + push[direction, 0, rows, cols]
                h_im = hold * (rate_re * h_im + rate_im * h_re) + push[direction, 1, rows, cols]
                h_re = new_re
                kept = kept * hold
            power_re, power_im = complex_power(rate_re, rate_im, steps)
            decay_re, decay_im = kept * power_re, kept * power_im
            for part, value in enumerate((h_re, h_im, decay_re, decay_im)):
                sub_ref[direction, part, :, cols] = value
            e_re = jnp.zeros((1, width), jnp.float32)
            e_im = jnp.zeros((1, width), jnp.float32)
            for j in order(SUBLANES, direction):
                d_re, d_im = decay_re[j : j + 1], decay_im[j : j + 1]
                e_re, e_im = (
                    d_re * e_re - d_im * e_im + h_re[j : j + 1],
                    d_re * e_im + d_im * e_re + h_im[j : j + 1],
                )
            put(direction, 0, column, e_re)
            put(direction, 1, column, e_im)


    copies = []
    for k in range(1, count):
        copy = pltpu.make_async_remote_copy(
            src_ref=ends_ref.at[(mine + k) // count],
            dst_ref=all_ref.at[mine],
            send_sem=send_sem.at[k],
            recv_sem=recv_sem.at[k],
            device_id={"sp": lax.rem(mine + k, count)},
            device_id_type=pl.DeviceIdType.MESH,
        )
        copy.start()
        copies.append(copy)
    all_ref[mine] = jnp.zeros(ends_ref.shape[1:], jnp.float32)

    late = [exchange(0, send_r, recv_r, r) for r in far[first:] + near]
    for copy in late:
        copy.start()
    for copy in copies:
        copy.wait()

    shares = jnp.concatenate(
        [all_ref[b, 6:7, :n_groups] for b in range(count)], axis=0
    )
    shares = jnp.concatenate(split3(shares), axis=1)
    for pack in packs:
        which, number, column, width, states = pack
        cols = slice(column, column + width)
        line, start = column // span, column % span
        kept = jnp.dot(
            shares, owners(pack, groups, n_groups, channels), preferred_element_type=jnp.float32
        )
        for direction in range(2):
            rate_re, rate_im = rates[direction, column]
            power_re, power_im = complex_power(rate_re, rate_im, tokens)
            c_re = jnp.zeros((1, width), jnp.float32)
            c_im = jnp.zeros((1, width), jnp.float32)
            for b in order(count, direction):
                use = b < mine if direction == 0 else b > mine
                e_re = all_ref[b, line : line + 1, start : start + width]
                e_im = all_ref[b, 3 + line : 4 + line, start : start + width]
                d_re, d_im = kept[b : b + 1] * power_re, kept[b : b + 1] * power_im
                c_re, c_im = (
                    jnp.where(use, d_re * c_re - d_im * c_im + e_re, c_re),
                    jnp.where(use, d_re * c_im + d_im * c_re + e_im, c_im),
                )
            for j in order(SUBLANES, direction):
                carry[direction, 0, j : j + 1, cols] = c_re
                carry[direction, 1, j : j + 1, cols] = c_im
                d_re = sub_ref[direction, 2, j : j + 1, cols]
                d_im = sub_ref[direction, 3, j : j + 1, cols]
                c_re, c_im = (
                    d_re * c_re - d_im * c_im + sub_ref[direction, 0, j : j + 1, cols],
                    d_re * c_im + d_im * c_re + sub_ref[direction, 1, j : j + 1, cols],
                )
    out_maps = (wide_out, narrow_out)
    for pack in packs:
        which, number, column, width, states = pack
        cols = slice(column, column + width)
        at = slice(number * per, (number + 1) * per)
        lanes = slice(which * half + number * LANES, which * half + (number + 1) * LANES)
        local = slice(number * LANES, (number + 1) * LANES)
        read = None
        for direction in range(2):
            rate_re, rate_im = rates[direction, column]
            h_re = carry[direction, 0, :, cols]
            h_im = carry[direction, 1, :, cols]
            for step in order(steps, direction):
                rows = slice(step * SUBLANES, (step + 1) * SUBLANES)
                hold = keep[direction, rows, cols]
                new_re = hold * (rate_re * h_re - rate_im * h_im) + push[direction, 0, rows, cols]
                h_im = hold * (rate_re * h_im + rate_im * h_re) + push[direction, 1, rows, cols]
                h_re = new_re
                push[direction, 0, rows, cols] = h_re
                push[direction, 1, rows, cols] = h_im
            for part in range(2):
                rows = out_maps[which][direction, part, at].reshape(LANES, states)
                if part:
                    rows = -rows
                term = lax.dot_general(
                    push[direction, part, :, cols].astype(jnp.bfloat16),
                    block_diagonal(rows, channels, states),
                    (((1,), (1,)), ((), ())),
                    preferred_element_type=jnp.float32,
                )
                read = term if read is None else read + term
        shaped = read + skip_ref[which : which + 1, local].astype(jnp.float32) * signal[
            :, lanes
        ].astype(jnp.float32)
        active = jax.nn.gelu(shaped, approximate=True)
        gate = block_diagonal(
            gate_ref[which, at].astype(jnp.float32).reshape(LANES, channels), channels, channels
        )
        opened = jax.nn.sigmoid(
            jnp.dot(active.astype(jnp.bfloat16), gate, preferred_element_type=jnp.float32)
        )
        mixed[:, lanes] = jnp.dot(
            unweave, (active * opened).astype(jnp.bfloat16), preferred_element_type=jnp.float32
        ).astype(jnp.bfloat16)
    rows = tokens // n_tp
    swaps = []
    for k in range(1, n_tp):
        other = lax.rem(tp + k, n_tp)
        copy = pltpu.make_async_remote_copy(
            src_ref=mixed.at[pl.ds(pl.multiple_of(other * rows, rows), rows)],
            dst_ref=out_ref.at[tp],
            send_sem=swap_sem.at[0, k],
            recv_sem=swap_sem.at[1, k],
            device_id={"tp": other},
            device_id_type=pl.DeviceIdType.MESH,
        )
        copy.start()
        swaps.append(copy)
    out_ref[tp] = mixed[pl.ds(pl.multiple_of(tp * rows, rows), rows), :]
    for copy in swaps:
        copy.wait()


    parts = [
        (out_ref[k, :, which * half : (which + 1) * half], which, k)
        for which in range(2) for k in range(n_tp)
    ]
    joined = jnp.concatenate([value.astype(jnp.float32) for value, _, _ in parts], axis=1)
    scale = rms_scale(joined, joined.shape[1])
    moved = (joined * scale * mixer_gain[...]).astype(jnp.bfloat16)
    send_m[...] = sections(moved)
    recv_m[0] = send_m[0]
    order_m = far + near
    outs = [exchange(1, send_m, recv_m, r) for r in order_m]
    for copy in outs:
        copy.start()
    share = route_weights[...]
    total_share = share[:, 0:1]
    for k in range(1, share.shape[1]):
        total_share = total_share + share[:, k : k + 1]
    weight = jnp.zeros((own_rows, slots), jnp.float32)
    for k, each in enumerate(picked):
        weight = weight + jnp.where(
            jnp.logical_and(each, here), share[:, k : k + 1] / total_share, 0.0
        )
    high = weight.astype(jnp.bfloat16)
    weights = jnp.concatenate([high, (weight - high.astype(jnp.float32)).astype(jnp.bfloat16)], axis=0)
    loads[0].wait()

    def own_hidden(cols):
        value = residual[:, cols].astype(jnp.float32) + jnp.dot(
            moved, out_w[:, cols], preferred_element_type=jnp.float32
        )
        own[:, cols] = value.astype(jnp.bfloat16).astype(jnp.float32)

    tiles(model, 512, own_hidden)
    for copy in loads[1:]:
        copy.wait()
    backs = []
    for a, b in chunks_of(devices):
        for r in range(max(a, 1), b):
            exchange(0, send_r, recv_r, r).wait_recv()
            exchange(1, send_m, recv_m, r).wait_recv()
        rows = (b - a) * capacity
        arrived = recv_m[a:b].astype(jnp.float32).reshape(rows, -1).astype(jnp.bfloat16)

        def full_hidden(cols, a=a, b=b, rows=rows, arrived=arrived):
            value = recv_r[a:b, :, cols].astype(jnp.float32).reshape(rows, -1) + jnp.dot(
                arrived, out_w[:, cols], preferred_element_type=jnp.float32
            )
            hidden[:rows, cols] = value.astype(jnp.bfloat16).astype(jnp.float32)

        tiles(model, 512, full_hidden)
        value = hidden[:rows, :]
        normed[:rows, :] = (value * rms_scale(value, model) * ffn_gain[...]).astype(jnp.bfloat16)

        def up(cols, rows=rows):
            value = normed[:rows, :]
            gate_val = jnp.dot(value, gate_w[:, cols], preferred_element_type=jnp.float32)
            up_val = jnp.dot(value, up_w[:, cols], preferred_element_type=jnp.float32)
            inner[:rows, cols] = (jax.nn.silu(gate_val) * up_val).astype(jnp.bfloat16)

        tiles(inner.shape[1], 256, up)

        def down(cols, a=a, b=b, rows=rows):
            value = jnp.dot(inner[:rows, :], down_w[:, cols], preferred_element_type=jnp.float32)
            send_o[a:b, :, cols] = value.reshape(b - a, capacity, -1).astype(jnp.bfloat16)

        tiles(model, 512, down)
        if a == 0:
            recv_o[0] = send_o[0]
        for r in range(max(a, 1), b):
            copy = exchange(2, send_o, recv_o, r)
            copy.start()
            backs.append(copy)
    for a, b in chunks_of(devices):
        for r in range(max(a, 1), b):
            exchange(2, send_o, recv_o, r).wait_recv()
        cut = weights[:, a * capacity : b * capacity]

        def gather(cols, a=a, b=b, cut=cut):
            rows = recv_o[a:b, :, cols].astype(jnp.float32)
            rows = rows.reshape((b - a) * capacity, -1).astype(jnp.bfloat16)
            both = jnp.dot(cut, rows, preferred_element_type=jnp.float32)
            own[:, cols] = own[:, cols] + (both[:own_rows] + both[own_rows:])

        tiles(model, 512, gather)
    result[...] = own[...].astype(jnp.bfloat16)
    for copy in early + late + outs + backs:
        copy.wait_send()


def local(*args):
    args = list(args)
    names = (
        "wide_inputs", "narrow_inputs", "wide_poles", "narrow_poles", "step_sizes", "forget",
        "wide_in_map", "narrow_in_map", "wide_out_map", "narrow_out_map", "skip_weight",
        "gate_mix", "residual", "mixer_gain", "out_proj", "ffn_gain", "routes", "route_weights",
        "gate_proj", "up_proj", "down_proj",
    )
    by = dict(zip(names, args))
    by["mixer_gain"] = by["mixer_gain"].reshape(1, -1)
    by["ffn_gain"] = by["ffn_gain"].reshape(1, -1)
    small = [by[n] for n in names if n not in ("gate_proj", "up_proj", "down_proj", "out_proj") and n not in ("mixer_gain", "ffn_gain", "routes", "route_weights")]
    small += [by[n] for n in ("mixer_gain", "ffn_gain", "routes", "route_weights")]
    big = [by[n] for n in ("gate_proj", "up_proj", "down_proj", "out_proj")]
    tokens, half = by["wide_inputs"].shape
    groups, channels, wide_state = by["wide_in_map"].shape[2:]
    narrow_state = by["narrow_in_map"].shape[4]
    _, total = pack_list(channels, groups, (wide_state, narrow_state))
    count, n_tp = lax.axis_size("sp"), lax.axis_size("tp")
    devices = count * n_tp
    own_rows, width = by["residual"].shape
    hidden_width = by["gate_proj"].shape[2]
    capacity = max(4 * tokens // (n_tp * devices), SUBLANES)
    joined = 2 * half * n_tp
    span = total // 3
    chunk = max(b - a for a, b in chunks_of(devices)) * capacity
    vmem = pl.BlockSpec(memory_space=pltpu.VMEM)
    hbm = pl.BlockSpec(memory_space=pltpu.HBM)
    f32, bf16 = jnp.float32, jnp.bfloat16
    dma = pltpu.SemaphoreType.DMA
    return pl.pallas_call(
        layer_kernel,
        out_shape=jax.ShapeDtypeStruct((own_rows, width), bf16),
        in_specs=[hbm] * (len(small) + len(big)),
        out_specs=vmem,
        scratch_shapes=[pltpu.VMEM(x.shape, x.dtype) for x in small]
        + [pltpu.VMEM(x.shape[-2:], x.dtype) for x in big]
        + [
            pltpu.VMEM((tokens, 2 * half), bf16),
            pltpu.VMEM((2, 2, tokens, total), f32),
            pltpu.VMEM((2, tokens, total), f32),
            pltpu.VMEM((2, 8, span), f32),
            pltpu.VMEM((2, 4, SUBLANES, total), f32),
            pltpu.VMEM((count, 8, span), f32),
            pltpu.VMEM((2, 2, SUBLANES, total), f32),
            pltpu.VMEM((tokens, 2 * half), bf16),
            pltpu.VMEM((n_tp, own_rows, 2 * half), bf16),
            pltpu.VMEM((devices, capacity, width), bf16),
            pltpu.VMEM((devices, capacity, width), bf16),
            pltpu.VMEM((devices, capacity, joined), bf16),
            pltpu.VMEM((devices, capacity, joined), bf16),
            pltpu.VMEM((devices, capacity, width), bf16),
            pltpu.VMEM((devices, capacity, width), bf16),
            pltpu.VMEM((own_rows, width), f32),
            pltpu.VMEM((chunk, width), f32),
            pltpu.VMEM((chunk, width), bf16),
            pltpu.VMEM((chunk, hidden_width), bf16),
            dma((len(small),)),
            dma((4,)),
            dma((count,)),
            dma((count,)),
            dma((2, n_tp)),
            dma((3, devices)),
            dma((3, devices)),
        ],
        compiler_params=pltpu.CompilerParams(
            collective_id=0, has_side_effects=True, vmem_limit_bytes=60 << 20
        ),
        name="layer",
    )(*small, *big)


def solution(mesh):
    return jax.shard_map(
        local,
        mesh=mesh,
        in_specs=(
            P("sp", "tp"),
            P("sp", "tp"),
            P(None, None, "tp", None),
            P(None, None, "tp", None),
            P(None, None, "tp"),
            P(None, None, "tp", "sp"),
            P(None, None, "tp", None, None),
            P(None, None, "tp", None, None),
            P(None, None, "tp", None, None),
            P(None, None, "tp", None, None),
            P(None, "tp"),
            P(None, "tp", None, None),
            P(("sp", "tp"), None),
            P(),
            P(),
            P(),
            P(("sp", "tp"), None),
            P(("sp", "tp"), None),
            P(("sp", "tp"), None, None),
            P(("sp", "tp"), None, None),
            P(("sp", "tp"), None, None),
        ),
        out_specs=P(("sp", "tp"), None),
        check_vma=False,
    )
```

```python
import jax
import jax.numpy as jnp
from jax import lax
from jax.experimental import pallas as pl
from jax.experimental.pallas import tpu as pltpu
from jax.sharding import PartitionSpec as P

epsilon = 1e-06
SUBLANES = 8
LANES = 128


def complex_power(re, im, exponent):
    out_re, out_im = None, None
    while exponent:
        if exponent & 1:
            if out_re is None:
                out_re, out_im = re, im
            else:
                out_re, out_im = out_re * re - out_im * im, out_re * im + out_im * re
        re, im = re * re - im * im, 2.0 * re * im
        exponent >>= 1
    return out_re, out_im


def pack_list(channels, groups, sets):
    per = LANES // channels
    packs, column = [], 0
    for which, states in enumerate(sets):
        for pack in range(groups // per):
            packs.append((which, pack, column, per * states, states))
            column += per * states
    return packs, column


def order(count, direction):
    return range(count) if direction == 0 else range(count - 1, -1, -1)


def widen(rows, copies):
    return jnp.concatenate([rows] * copies, axis=1)


def block_diagonal(rows, channels, states):
    copies = LANES // channels
    tiled = widen(rows, copies)
    row = lax.broadcasted_iota(jnp.int32, tiled.shape, 0) // channels
    column = lax.broadcasted_iota(jnp.int32, tiled.shape, 1) // states
    return jnp.where(row == column, tiled, 0.0).astype(jnp.bfloat16)


def flat_row(rows, states):
    copies = rows.shape[0]
    tiled = widen(rows, copies)
    row = lax.broadcasted_iota(jnp.int32, tiled.shape, 0)
    column = lax.broadcasted_iota(jnp.int32, tiled.shape, 1) // states
    return jnp.sum(jnp.where(row == column, tiled, 0.0), axis=0, keepdims=True)


def split3(value):
    high = value.astype(jnp.bfloat16)
    rest = value - high.astype(jnp.float32)
    mid = rest.astype(jnp.bfloat16)
    low = (rest - mid.astype(jnp.float32)).astype(jnp.bfloat16)
    return high, mid, low


def owners(pack, groups, count, channels):
    which, number, _, width, states = pack
    first = which * groups + number * (LANES // channels)
    row = lax.broadcasted_iota(jnp.int32, (3 * count, width), 0) % count
    column = first + lax.broadcasted_iota(jnp.int32, (3 * count, width), 1) // states
    return jnp.where(row == column, 1.0, 0.0).astype(jnp.bfloat16)


def flip(value, bits):
    bit = 1
    while bit <= bits:
        if bits & bit:
            value = value + bit - 2 * bit * ((value // bit) % 2)
        bit *= 2
    return value


def rms_scale(value, width):
    return lax.rsqrt(jnp.sum(value * value, axis=1, keepdims=True) / width + epsilon)


def tiles(width, tile, step):
    full = width // tile
    if full:

        @pl.loop(0, full)
        def _(j):
            step(pl.ds(pl.multiple_of(j * tile, tile), tile))

    if width % tile:
        step(slice(full * tile, width))


def chunks_of(devices):
    near, far = min(16, devices // 2), min(16, devices // 4)
    half = devices // 2
    return [(a, a + near) for a in range(0, half, near)] + [
        (a, a + far) for a in range(half, devices, far)
    ]


def send_order(devices):
    half, quarter = devices // 2, devices // 4
    first = list(range(half, half + quarter))
    near = list(range(1, half))
    return first + near + list(range(half + quarter, devices))


N_SMALL = 17


def layer_kernel(*refs):
    small_hbm, refs = refs[:N_SMALL], refs[N_SMALL:]
    big_hbm, refs = refs[:4], refs[4:]
    result, refs = refs[0], refs[1:]
    small, refs = refs[:N_SMALL], refs[N_SMALL:]
    big, refs = refs[:4], refs[4:]
    (
        wide_u, narrow_u, wide_poles, narrow_poles, step_ref, forget_ref, wide_in, narrow_in,
        wide_out, narrow_out, skip_ref, gate_ref, residual, mixer_gain, ffn_gain, routes,
        route_weights,
    ) = small
    gate_w, up_w, down_w, out_w = big
    (
        signal, push, keep, ends_ref, sub_ref, all_ref, carry, mixed, out_ref, send_d, recv_d,
        send_o, recv_o, own, normed, inner,
        small_sem, big_sem, send_sem, recv_sem, swap_sem, send_sems, recv_sems,
    ) = refs
    tokens, half = wide_u.shape
    groups, channels = wide_in.shape[2:4]
    sets = (wide_in.shape[4], narrow_in.shape[4])
    packs, total = pack_list(channels, groups, sets)
    per = LANES // channels
    steps = tokens // SUBLANES
    span = ends_ref.shape[2]
    count = lax.axis_size("sp")
    n_tp = lax.axis_size("tp")
    mine = lax.axis_index("sp")
    tp = lax.axis_index("tp")
    devices, capacity, model = send_d.shape
    own_rows = residual.shape[0]
    others = [(r // n_tp, r % n_tp) for r in range(devices)]
    peers = [{"sp": flip(mine, a), "tp": flip(tp, b)} for a, b in others]
    barrier = pltpu.get_barrier_semaphore()
    for r in range(1, devices):
        pl.semaphore_signal(
            barrier, inc=1, device_id=peers[r], device_id_type=pl.DeviceIdType.MESH
        )
    stages = []
    for i in (0, 1, 5, 2, 3, 4, 6, 7, 8, 9, 10, 11, 12, 13, 14, 15, 16):
        copy = pltpu.make_async_copy(small_hbm[i], small[i], small_sem.at[i])
        copy.start()
        stages.append(copy)
    loads = []
    for i in (3, 0, 1, 2):
        source = big_hbm[i] if i == 3 else big_hbm[i].at[0]
        loads.append(pltpu.make_async_copy(source, big[i], big_sem.at[i]))

    def exchange(which, source, target, r):
        return pltpu.make_async_remote_copy(
            src_ref=source.at[r], dst_ref=target.at[r],
            send_sem=send_sems.at[which, r], recv_sem=recv_sems.at[which, r],
            device_id=peers[r], device_id_type=pl.DeviceIdType.MESH,
        )

    for copy in stages:
        copy.wait()
    for copy in loads:
        copy.start()

    row = lax.broadcasted_iota(jnp.int32, (tokens, tokens), 0)
    column = lax.broadcasted_iota(jnp.int32, (tokens, tokens), 1)
    weave = jnp.where(
        column == (row % SUBLANES) * steps + row // SUBLANES, 1.0, 0.0
    ).astype(jnp.bfloat16)
    unweave = jnp.where(
        row == (column % SUBLANES) * steps + column // SUBLANES, 1.0, 0.0
    ).astype(jnp.bfloat16)
    inputs = (wide_u, narrow_u)
    for which in range(2):
        signal[:, which * half : (which + 1) * half] = jnp.dot(
            weave, inputs[which][...], preferred_element_type=jnp.float32
        ).astype(jnp.bfloat16)
    held = []
    n_groups = 2 * groups
    for direction in range(2):
        rows = jnp.concatenate([forget_ref[direction, 0], forget_ref[direction, 1]], axis=0)
        pieces = jnp.concatenate(split3(jnp.exp(-rows)), axis=0)
        held.append(
            lax.dot_general(
                weave, pieces, (((1,), (1,)), ((), ())), preferred_element_type=jnp.float32
            ).astype(jnp.bfloat16)
        )
        sums = lax.dot_general(
            jnp.ones((SUBLANES, tokens), jnp.float32), rows, (((1,), (1,)), ((), ())),
            precision=lax.Precision.HIGHEST, preferred_element_type=jnp.float32,
        )
        ends_ref[direction, 6:8, :] = jnp.zeros((2, span), jnp.float32)
        ends_ref[direction, 6:7, :n_groups] = jnp.exp(-sums[:1])

    def put(direction, part, column, value):
        done = 0
        while done < value.shape[1]:
            at = column + done
            line, start = at // span, at % span
            size = min(value.shape[1] - done, span - start)
            ends_ref[direction, 3 * part + line : 3 * part + line + 1, start : start + size] = (
                value[:, done : done + size]
            )
            done += size

    eye_row = lax.broadcasted_iota(jnp.int32, (per, groups), 0)
    eye_column = lax.broadcasted_iota(jnp.int32, (per, groups), 1)
    poles, in_maps = (wide_poles, narrow_poles), (wide_in, narrow_in)
    rates = {}
    for pack in packs:
        which, number, column, width, states = pack
        cols = slice(column, column + width)
        at = slice(number * per, (number + 1) * per)
        lanes = slice(which * half + number * LANES, which * half + (number + 1) * LANES)
        owner = owners(pack, groups, n_groups, channels)
        for direction in range(2):
            re, im = poles[which][direction, 0, at, :], poles[which][direction, 1, at, :]
            growth = jnp.exp(re)
            rate_re, rate_im = growth * jnp.cos(im), growth * jnp.sin(im)
            numer = rate_re - 1.0
            step = jnp.sum(
                jnp.where(
                    eye_column == eye_row + number * per,
                    step_ref[direction, which : which + 1, :], 0.0,
                ),
                axis=1, keepdims=True,
            )
            scale = step / (re * re + im * im)
            factor_re = ((numer * re + rate_im * im) * scale)[:, None, :]
            factor_im = ((rate_im * re - numer * im) * scale)[:, None, :]
            in_re, in_im = in_maps[which][direction, 0, at], in_maps[which][direction, 1, at]
            enter = (factor_re * in_re - factor_im * in_im, factor_re * in_im + factor_im * in_re)
            for part in range(2):
                push[direction, part, :, cols] = jnp.dot(
                    signal[:, lanes],
                    block_diagonal(enter[part].reshape(LANES, states), channels, states),
                    preferred_element_type=jnp.float32,
                )
            keep[direction, :, cols] = jnp.dot(
                held[direction], owner, preferred_element_type=jnp.float32
            )
            rate_re, rate_im = flat_row(rate_re, states), flat_row(rate_im, states)
            rates[direction, column] = (rate_re, rate_im)
            h_re = jnp.zeros((SUBLANES, width), jnp.float32)
            h_im = jnp.zeros((SUBLANES, width), jnp.float32)
            kept = jnp.ones((SUBLANES, width), jnp.float32)
            for step in order(steps, direction):
                rows = slice(step * SUBLANES, (step + 1) * SUBLANES)
                hold = keep[direction, rows, cols]
                new_re = hold * (rate_re * h_re - rate_im * h_im) + push[direction, 0, rows, cols]
                h_im = hold * (rate_re * h_im + rate_im * h_re) + push[direction, 1, rows, cols]
                h_re = new_re
                kept = kept * hold
            power_re, power_im = complex_power(rate_re, rate_im, steps)
            decay_re, decay_im = kept * power_re, kept * power_im
            for part, value in enumerate((h_re, h_im, decay_re, decay_im)):
                sub_ref[direction, part, :, cols] = value
            e_re = jnp.zeros((1, width), jnp.float32)
            e_im = jnp.zeros((1, width), jnp.float32)
            for j in order(SUBLANES, direction):
                d_re, d_im = decay_re[j : j + 1], decay_im[j : j + 1]
                e_re, e_im = (
                    d_re * e_re - d_im * e_im + h_re[j : j + 1],
                    d_re * e_im + d_im * e_re + h_im[j : j + 1],
                )
            put(direction, 0, column, e_re)
            put(direction, 1, column, e_im)


    pl.semaphore_wait(barrier, devices - 1)
    copies = []
    for k in range(1, count):
        copy = pltpu.make_async_remote_copy(
            src_ref=ends_ref.at[(mine + k) // count],
            dst_ref=all_ref.at[mine],
            send_sem=send_sem.at[k],
            recv_sem=recv_sem.at[k],
            device_id={"sp": lax.rem(mine + k, count)},
            device_id_type=pl.DeviceIdType.MESH,
        )
        copy.start()
        copies.append(copy)
    all_ref[mine] = jnp.zeros(ends_ref.shape[1:], jnp.float32)

    slots = devices * capacity
    slot = lax.broadcasted_iota(jnp.int32, (slots, own_rows), 0)
    expert = (slot // capacity) ^ (mine * n_tp + tp)
    picked = [routes[k : k + 1, :] == expert for k in range(routes.shape[0])]
    chosen = picked[0]
    for each in picked[1:]:
        chosen = jnp.logical_or(chosen, each)
    chosen = jnp.where(chosen, 1.0, 0.0)
    earlier = jnp.where(
        lax.broadcasted_iota(jnp.int32, (own_rows, own_rows), 0)
        < lax.broadcasted_iota(jnp.int32, (own_rows, own_rows), 1),
        1.0, 0.0,
    ).astype(jnp.bfloat16)
    rank = jnp.dot(chosen.astype(jnp.bfloat16), earlier, preferred_element_type=jnp.float32)
    here = rank == (slot % capacity).astype(jnp.float32)
    spot = jnp.where(here, chosen, 0.0).astype(jnp.bfloat16)
    share = route_weights[...]
    total_share = share[0:1]
    for k in range(1, share.shape[0]):
        total_share = total_share + share[k : k + 1]
    weight = jnp.zeros((slots, own_rows), jnp.float32)
    for k, each in enumerate(picked):
        weight = weight + jnp.where(
            jnp.logical_and(each, here), share[k : k + 1] / total_share, 0.0
        )
    weight = weight.T
    high = weight.astype(jnp.bfloat16)
    weights = jnp.concatenate(
        [high, (weight - high.astype(jnp.float32)).astype(jnp.bfloat16)], axis=0
    )
    for copy in copies:
        copy.wait()

    shares = jnp.concatenate(
        [all_ref[b, 6:7, :n_groups] for b in range(count)], axis=0
    )
    shares = jnp.concatenate(split3(shares), axis=1)
    for pack in packs:
        which, number, column, width, states = pack
        cols = slice(column, column + width)
        line, start = column // span, column % span
        kept = jnp.dot(
            shares, owners(pack, groups, n_groups, channels), preferred_element_type=jnp.float32
        )
        for direction in range(2):
            rate_re, rate_im = rates[direction, column]
            power_re, power_im = complex_power(rate_re, rate_im, tokens)
            c_re = jnp.zeros((1, width), jnp.float32)
            c_im = jnp.zeros((1, width), jnp.float32)
            for b in order(count, direction):
                use = b < mine if direction == 0 else b > mine
                e_re = all_ref[b, line : line + 1, start : start + width]
                e_im = all_ref[b, 3 + line : 4 + line, start : start + width]
                d_re, d_im = kept[b : b + 1] * power_re, kept[b : b + 1] * power_im
                c_re, c_im = (
                    jnp.where(use, d_re * c_re - d_im * c_im + e_re, c_re),
                    jnp.where(use, d_re * c_im + d_im * c_re + e_im, c_im),
                )
            for j in order(SUBLANES, direction):
                carry[direction, 0, j : j + 1, cols] = c_re
                carry[direction, 1, j : j + 1, cols] = c_im
                d_re = sub_ref[direction, 2, j : j + 1, cols]
                d_im = sub_ref[direction, 3, j : j + 1, cols]
                c_re, c_im = (
                    d_re * c_re - d_im * c_im + sub_ref[direction, 0, j : j + 1, cols],
                    d_re * c_im + d_im * c_re + sub_ref[direction, 1, j : j + 1, cols],
                )
    out_maps = (wide_out, narrow_out)
    for pack in packs:
        which, number, column, width, states = pack
        cols = slice(column, column + width)
        at = slice(number * per, (number + 1) * per)
        lanes = slice(which * half + number * LANES, which * half + (number + 1) * LANES)
        local = slice(number * LANES, (number + 1) * LANES)
        read = None
        for direction in range(2):
            rate_re, rate_im = rates[direction, column]
            h_re = carry[direction, 0, :, cols]
            h_im = carry[direction, 1, :, cols]
            for step in order(steps, direction):
                rows = slice(step * SUBLANES, (step + 1) * SUBLANES)
                hold = keep[direction, rows, cols]
                new_re = hold * (rate_re * h_re - rate_im * h_im) + push[direction, 0, rows, cols]
                h_im = hold * (rate_re * h_im + rate_im * h_re) + push[direction, 1, rows, cols]
                h_re = new_re
                push[direction, 0, rows, cols] = h_re
                push[direction, 1, rows, cols] = h_im
            for part in range(2):
                rows = out_maps[which][direction, part, at].reshape(LANES, states)
                if part:
                    rows = -rows
                term = lax.dot_general(
                    push[direction, part, :, cols].astype(jnp.bfloat16),
                    block_diagonal(rows, channels, states),
                    (((1,), (1,)), ((), ())),
                    preferred_element_type=jnp.float32,
                )
                read = term if read is None else read + term
        shaped = read + skip_ref[which : which + 1, local].astype(jnp.float32) * signal[
            :, lanes
        ].astype(jnp.float32)
        active = jax.nn.gelu(shaped, approximate=True)
        gate = block_diagonal(
            gate_ref[which, at].astype(jnp.float32).reshape(LANES, channels), channels, channels
        )
        opened = jax.nn.sigmoid(
            jnp.dot(active.astype(jnp.bfloat16), gate, preferred_element_type=jnp.float32)
        )
        mixed[:, lanes] = jnp.dot(
            unweave, (active * opened).astype(jnp.bfloat16), preferred_element_type=jnp.float32
        ).astype(jnp.bfloat16)
    rows = tokens // n_tp
    swaps = []
    for k in range(1, n_tp):
        other = lax.rem(tp + k, n_tp)
        copy = pltpu.make_async_remote_copy(
            src_ref=mixed.at[pl.ds(pl.multiple_of(other * rows, rows), rows)],
            dst_ref=out_ref.at[tp],
            send_sem=swap_sem.at[0, k],
            recv_sem=swap_sem.at[1, k],
            device_id={"tp": other},
            device_id_type=pl.DeviceIdType.MESH,
        )
        copy.start()
        swaps.append(copy)
    out_ref[tp] = mixed[pl.ds(pl.multiple_of(tp * rows, rows), rows), :]
    for copy in swaps:
        copy.wait()


    parts = [
        (out_ref[k, :, which * half : (which + 1) * half], which, k)
        for which in range(2) for k in range(n_tp)
    ]
    joined = jnp.concatenate([value.astype(jnp.float32) for value, _, _ in parts], axis=1)
    scale = rms_scale(joined, joined.shape[1])
    moved = (joined * scale * mixer_gain[...]).astype(jnp.bfloat16)
    loads[0].wait()

    def own_hidden(cols):
        value = residual[:, cols].astype(jnp.float32) + jnp.dot(
            moved, out_w[:, cols], preferred_element_type=jnp.float32
        )
        own[:, cols] = value.astype(jnp.bfloat16).astype(jnp.float32)

    tiles(model, 512, own_hidden)
    scale = rms_scale(own[...], model)

    def dispatch(cols):
        value = (own[:, cols] * scale * ffn_gain[:, cols]).astype(jnp.bfloat16)
        rows = jnp.dot(spot, value, preferred_element_type=jnp.float32)
        send_d[:, :, cols] = rows.reshape(devices, capacity, -1).astype(jnp.bfloat16)

    tiles(model, 512, dispatch)
    recv_d[0] = send_d[0]
    outs = [exchange(0, send_d, recv_d, r) for r in send_order(devices)]
    for copy in outs:
        copy.start()
    for copy in loads[1:]:
        copy.wait()
    backs = []
    for a, b in chunks_of(devices):
        for r in range(max(a, 1), b):
            exchange(0, send_d, recv_d, r).wait_recv()
        rows = (b - a) * capacity

        def arrange(cols, a=a, b=b, rows=rows):
            value = recv_d[a:b, :, cols].astype(jnp.float32).reshape(rows, -1)
            normed[:rows, cols] = value.astype(jnp.bfloat16)

        tiles(model, 512, arrange)

        def up(cols, rows=rows):
            value = normed[:rows, :]
            gate_val = jnp.dot(value, gate_w[:, cols], preferred_element_type=jnp.float32)
            up_val = jnp.dot(value, up_w[:, cols], preferred_element_type=jnp.float32)
            inner[:rows, cols] = (jax.nn.silu(gate_val) * up_val).astype(jnp.bfloat16)

        tiles(inner.shape[1], 256, up)

        def down(cols, a=a, b=b, rows=rows):
            value = jnp.dot(inner[:rows, :], down_w[:, cols], preferred_element_type=jnp.float32)
            send_o[a:b, :, cols] = value.reshape(b - a, capacity, -1).astype(jnp.bfloat16)

        tiles(model, 512, down)
        if a == 0:
            recv_o[0] = send_o[0]
        for r in range(max(a, 1), b):
            copy = exchange(1, send_o, recv_o, r)
            copy.start()
            backs.append(copy)
    for a, b in chunks_of(devices):
        for r in range(max(a, 1), b):
            exchange(1, send_o, recv_o, r).wait_recv()
        part = weights[:, a * capacity : b * capacity]

        def gather(cols, a=a, b=b, part=part):
            rows = recv_o[a:b, :, cols].astype(jnp.float32)
            rows = rows.reshape((b - a) * capacity, -1).astype(jnp.bfloat16)
            both = jnp.dot(part, rows, preferred_element_type=jnp.float32)
            own[:, cols] = own[:, cols] + (both[:own_rows] + both[own_rows:])

        tiles(model, 512, gather)
    result[...] = own[...].astype(jnp.bfloat16)
    for copy in outs + backs:
        copy.wait_send()


def local(*args):
    args = list(args)
    names = (
        "wide_inputs", "narrow_inputs", "wide_poles", "narrow_poles", "step_sizes", "forget",
        "wide_in_map", "narrow_in_map", "wide_out_map", "narrow_out_map", "skip_weight",
        "gate_mix", "residual", "mixer_gain", "out_proj", "ffn_gain", "routes", "route_weights",
        "gate_proj", "up_proj", "down_proj",
    )
    by = dict(zip(names, args))
    by["mixer_gain"] = by["mixer_gain"].reshape(1, -1)
    by["ffn_gain"] = by["ffn_gain"].reshape(1, -1)
    by["routes"] = by["routes"].T
    by["route_weights"] = by["route_weights"].T
    small = [by[n] for n in names if n not in ("gate_proj", "up_proj", "down_proj", "out_proj") and n not in ("mixer_gain", "ffn_gain", "routes", "route_weights")]
    small += [by[n] for n in ("mixer_gain", "ffn_gain", "routes", "route_weights")]
    big = [by[n] for n in ("gate_proj", "up_proj", "down_proj", "out_proj")]
    tokens, half = by["wide_inputs"].shape
    groups, channels, wide_state = by["wide_in_map"].shape[2:]
    narrow_state = by["narrow_in_map"].shape[4]
    _, total = pack_list(channels, groups, (wide_state, narrow_state))
    count, n_tp = lax.axis_size("sp"), lax.axis_size("tp")
    devices = count * n_tp
    own_rows, width = by["residual"].shape
    hidden_width = by["gate_proj"].shape[2]
    capacity = max(4 * tokens // (n_tp * devices), SUBLANES)
    span = total // 3
    chunk = max(b - a for a, b in chunks_of(devices)) * capacity
    vmem = pl.BlockSpec(memory_space=pltpu.VMEM)
    hbm = pl.BlockSpec(memory_space=pltpu.HBM)
    f32, bf16 = jnp.float32, jnp.bfloat16
    dma = pltpu.SemaphoreType.DMA
    return pl.pallas_call(
        layer_kernel,
        out_shape=jax.ShapeDtypeStruct((own_rows, width), bf16),
        in_specs=[hbm] * (len(small) + len(big)),
        out_specs=vmem,
        scratch_shapes=[pltpu.VMEM(x.shape, x.dtype) for x in small]
        + [pltpu.VMEM(x.shape[-2:], x.dtype) for x in big]
        + [
            pltpu.VMEM((tokens, 2 * half), bf16),
            pltpu.VMEM((2, 2, tokens, total), f32),
            pltpu.VMEM((2, tokens, total), f32),
            pltpu.VMEM((2, 8, span), f32),
            pltpu.VMEM((2, 4, SUBLANES, total), f32),
            pltpu.VMEM((count, 8, span), f32),
            pltpu.VMEM((2, 2, SUBLANES, total), f32),
            pltpu.VMEM((tokens, 2 * half), bf16),
            pltpu.VMEM((n_tp, own_rows, 2 * half), bf16),
            pltpu.VMEM((devices, capacity, width), bf16),
            pltpu.VMEM((devices, capacity, width), bf16),
            pltpu.VMEM((devices, capacity, width), bf16),
            pltpu.VMEM((devices, capacity, width), bf16),
            pltpu.VMEM((own_rows, width), f32),
            pltpu.VMEM((chunk, width), bf16),
            pltpu.VMEM((chunk, hidden_width), bf16),
            dma((len(small),)),
            dma((4,)),
            dma((count,)),
            dma((count,)),
            dma((2, n_tp)),
            dma((2, devices)),
            dma((2, devices)),
        ],
        compiler_params=pltpu.CompilerParams(
            collective_id=0, has_side_effects=True, vmem_limit_bytes=60 << 20
        ),
        name="layer",
    )(*small, *big)


def solution(mesh):
    return jax.shard_map(
        local,
        mesh=mesh,
        in_specs=(
            P("sp", "tp"),
            P("sp", "tp"),
            P(None, None, "tp", None),
            P(None, None, "tp", None),
            P(None, None, "tp"),
            P(None, None, "tp", "sp"),
            P(None, None, "tp", None, None),
            P(None, None, "tp", None, None),
            P(None, None, "tp", None, None),
            P(None, None, "tp", None, None),
            P(None, "tp"),
            P(None, "tp", None, None),
            P(("sp", "tp"), None),
            P(),
            P(),
            P(),
            P(("sp", "tp"), None),
            P(("sp", "tp"), None),
            P(("sp", "tp"), None, None),
            P(("sp", "tp"), None, None),
            P(("sp", "tp"), None, None),
        ),
        out_specs=P(("sp", "tp"), None),
        check_vma=False,
    )
```

```python
import jax
import jax.numpy as jnp
from jax import lax
from jax.experimental import pallas as pl
from jax.experimental.pallas import tpu as pltpu
from jax.sharding import PartitionSpec as P

epsilon = 1e-06
SUBLANES = 8
LANES = 128
TILE = 512


def complex_power(re, im, exponent):
    out_re, out_im = None, None
    while exponent:
        if exponent & 1:
            if out_re is None:
                out_re, out_im = re, im
            else:
                out_re, out_im = out_re * re - out_im * im, out_re * im + out_im * re
        re, im = re * re - im * im, 2.0 * re * im
        exponent >>= 1
    return out_re, out_im


def pack_list(channels, groups, sets):
    per = LANES // channels
    packs, column = [], 0
    for which, states in enumerate(sets):
        for pack in range(groups // per):
            packs.append((which, pack, column, per * states, states))
            column += per * states
    return packs, column


def order(count, direction):
    return range(count) if direction == 0 else range(count - 1, -1, -1)


def widen(rows, copies):
    return jnp.concatenate([rows] * copies, axis=1)


def block_diagonal(rows, channels, states):
    copies = LANES // channels
    tiled = widen(rows, copies)
    row = lax.broadcasted_iota(jnp.int32, tiled.shape, 0) // channels
    column = lax.broadcasted_iota(jnp.int32, tiled.shape, 1) // states
    return jnp.where(row == column, tiled, 0.0).astype(jnp.bfloat16)


def flat_row(rows, states):
    copies = rows.shape[0]
    tiled = widen(rows, copies)
    row = lax.broadcasted_iota(jnp.int32, tiled.shape, 0)
    column = lax.broadcasted_iota(jnp.int32, tiled.shape, 1) // states
    return jnp.sum(jnp.where(row == column, tiled, 0.0), axis=0, keepdims=True)


def split3(value):
    high = value.astype(jnp.bfloat16)
    rest = value - high.astype(jnp.float32)
    mid = rest.astype(jnp.bfloat16)
    low = (rest - mid.astype(jnp.float32)).astype(jnp.bfloat16)
    return high, mid, low


def owners(pack, groups, count, channels):
    which, number, _, width, states = pack
    first = which * groups + number * (LANES // channels)
    row = lax.broadcasted_iota(jnp.int32, (3 * count, width), 0) % count
    column = first + lax.broadcasted_iota(jnp.int32, (3 * count, width), 1) // states
    return jnp.where(row == column, 1.0, 0.0).astype(jnp.bfloat16)


def flip(value, bits):
    bit = 1
    while bit <= bits:
        if bits & bit:
            value = value + bit - 2 * bit * ((value // bit) % 2)
        bit *= 2
    return value


def rms_scale(value, width):
    return lax.rsqrt(jnp.sum(value * value, axis=1, keepdims=True) / width + epsilon)


def tiles(width, tile, step):
    full = width // tile
    if full:

        @pl.loop(0, full)
        def _(j):
            step(pl.ds(pl.multiple_of(j * tile, tile), tile))

    if width % tile:
        step(slice(full * tile, width))


def chunks_of(devices):
    near, far = min(16, devices // 2), min(16, devices // 4)
    half = devices // 2
    return [(a, a + near) for a in range(0, half, near)] + [
        (a, a + far) for a in range(half, devices, far)
    ]


def send_order(devices):
    half, quarter = devices // 2, devices // 4
    first = list(range(half, half + quarter))
    near = list(range(1, half))
    return first, near + list(range(half + quarter, devices))


N_SMALL = 17


def layer_kernel(*refs):
    small_hbm, refs = refs[:N_SMALL], refs[N_SMALL:]
    big_hbm, refs = refs[:4], refs[4:]
    result, refs = refs[0], refs[1:]
    small, refs = refs[:N_SMALL], refs[N_SMALL:]
    big, refs = refs[:4], refs[4:]
    (
        wide_u, narrow_u, wide_poles, narrow_poles, step_ref, forget_ref, wide_in, narrow_in,
        wide_out, narrow_out, skip_ref, gate_ref, residual, mixer_gain, ffn_gain, routes,
        route_weights,
    ) = small
    gate_w, up_w, down_w, out_w = big
    (
        signal, push, keep, ends_ref, ends_wide, sub_ref, all_ref, all_wide, carry, leave, gates, mixed, out_ref, send_d, recv_d,
        send_o, recv_o, own, normed, inner,
        small_sem, big_sem, send_sem, recv_sem, swap_sem, send_sems, recv_sems,
    ) = refs
    tokens, half = wide_u.shape
    groups, channels = wide_in.shape[2:4]
    sets = (wide_in.shape[4], narrow_in.shape[4])
    packs, total = pack_list(channels, groups, sets)
    per = LANES // channels
    steps = tokens // SUBLANES
    span = ends_ref.shape[2]
    count = lax.axis_size("sp")
    n_tp = lax.axis_size("tp")
    mine = lax.axis_index("sp")
    tp = lax.axis_index("tp")
    devices, capacity, model = send_d.shape
    own_rows = residual.shape[0]
    others = [(r // n_tp, r % n_tp) for r in range(devices)]
    peers = [{"sp": flip(mine, a), "tp": flip(tp, b)} for a, b in others]
    barrier = pltpu.get_barrier_semaphore()
    for r in range(1, devices):
        pl.semaphore_signal(
            barrier, inc=1, device_id=peers[r], device_id_type=pl.DeviceIdType.MESH
        )
    stages = []
    for i in (0, 1, 5, 2, 3, 4, 6, 7, 8, 9, 10, 11, 12, 13, 14, 15, 16):
        copy = pltpu.make_async_copy(small_hbm[i], small[i], small_sem.at[i])
        copy.start()
        stages.append(copy)
    loads = []
    for i in (3, 0, 1, 2):
        source = big_hbm[i] if i == 3 else big_hbm[i].at[0]
        loads.append(pltpu.make_async_copy(source, big[i], big_sem.at[i]))

    spans = chunks_of(devices)

    def group_of(r):
        return [a <= r < b for a, b in spans].index(True)

    def whole(which, source, target, first, last):
        at = pl.ds(first, last - first)
        return pltpu.make_async_remote_copy(
            src_ref=source.at[at], dst_ref=target.at[at],
            send_sem=send_sems.at[which], recv_sem=recv_sems.at[which, group_of(first)],
            device_id=peers[1], device_id_type=pl.DeviceIdType.MESH,
        )

    def exchange(which, source, target, r, part=None):
        at = (r,) if part is None else (r, slice(None), slice(part * TILE, (part + 1) * TILE))
        return pltpu.make_async_remote_copy(
            src_ref=source.at[at], dst_ref=target.at[at],
            send_sem=send_sems.at[which], recv_sem=recv_sems.at[which, group_of(r)],
            device_id=peers[r], device_id_type=pl.DeviceIdType.MESH,
        )

    for copy in stages[:8]:
        copy.wait()
    for copy in loads:
        copy.start()

    row = lax.broadcasted_iota(jnp.int32, (tokens, tokens), 0)
    column = lax.broadcasted_iota(jnp.int32, (tokens, tokens), 1)
    weave = jnp.where(
        column == (row % SUBLANES) * steps + row // SUBLANES, 1.0, 0.0
    ).astype(jnp.bfloat16)
    unweave = jnp.where(
        row == (column % SUBLANES) * steps + column // SUBLANES, 1.0, 0.0
    ).astype(jnp.bfloat16)
    inputs = (wide_u, narrow_u)
    for which in range(2):
        signal[:, which * half : (which + 1) * half] = jnp.dot(
            weave, inputs[which][...], preferred_element_type=jnp.float32
        ).astype(jnp.bfloat16)
    held = []
    n_groups = 2 * groups
    for direction in range(2):
        rows = jnp.concatenate([forget_ref[direction, 0], forget_ref[direction, 1]], axis=0)
        pieces = jnp.concatenate(split3(jnp.exp(-rows)), axis=0)
        held.append(
            lax.dot_general(
                weave, pieces, (((1,), (1,)), ((), ())), preferred_element_type=jnp.float32
            ).astype(jnp.bfloat16)
        )
        sums = lax.dot_general(
            jnp.ones((SUBLANES, tokens), jnp.float32), rows, (((1,), (1,)), ((), ())),
            precision=lax.Precision.HIGHEST, preferred_element_type=jnp.float32,
        )
        ends_wide[direction, 6:8, :] = jnp.zeros((2, span), jnp.float32)
        ends_wide[direction, 6:7, : 3 * n_groups] = jnp.concatenate(
            [piece.astype(jnp.float32) for piece in split3(jnp.exp(-sums))], axis=1
        )[:1]

    def put(direction, part, column, value):
        done = 0
        while done < value.shape[1]:
            at = column + done
            line, start = at // span, at % span
            size = min(value.shape[1] - done, span - start)
            ends_wide[direction, 3 * part + line : 3 * part + line + 1, start : start + size] = (
                value[:, done : done + size]
            )
            done += size

    eye_row = lax.broadcasted_iota(jnp.int32, (per, groups), 0)
    eye_column = lax.broadcasted_iota(jnp.int32, (per, groups), 1)
    poles, in_maps = (wide_poles, narrow_poles), (wide_in, narrow_in)
    rates = {}
    for pack in packs:
        which, number, column, width, states = pack
        cols = slice(column, column + width)
        at = slice(number * per, (number + 1) * per)
        lanes = slice(which * half + number * LANES, which * half + (number + 1) * LANES)
        owner = owners(pack, groups, n_groups, channels)
        for direction in range(2):
            re, im = poles[which][direction, 0, at, :], poles[which][direction, 1, at, :]
            growth = jnp.exp(re)
            rate_re, rate_im = growth * jnp.cos(im), growth * jnp.sin(im)
            numer = rate_re - 1.0
            step = jnp.sum(
                jnp.where(
                    eye_column == eye_row + number * per,
                    step_ref[direction, which : which + 1, :], 0.0,
                ),
                axis=1, keepdims=True,
            )
            scale = step / (re * re + im * im)
            factor_re = ((numer * re + rate_im * im) * scale)[:, None, :]
            factor_im = ((rate_im * re - numer * im) * scale)[:, None, :]
            in_re, in_im = in_maps[which][direction, 0, at], in_maps[which][direction, 1, at]
            enter = (factor_re * in_re - factor_im * in_im, factor_re * in_im + factor_im * in_re)
            for part in range(2):
                push[direction, part, :, cols] = jnp.dot(
                    signal[:, lanes],
                    block_diagonal(enter[part].reshape(LANES, states), channels, states),
                    preferred_element_type=jnp.float32,
                )
            keep[direction, :, cols] = jnp.dot(
                held[direction], owner, preferred_element_type=jnp.float32
            )
            rate_re, rate_im = flat_row(rate_re, states), flat_row(rate_im, states)
            rates[direction, column] = (rate_re, rate_im)
            h_re = jnp.zeros((SUBLANES, width), jnp.float32)
            h_im = jnp.zeros((SUBLANES, width), jnp.float32)
            kept = jnp.ones((SUBLANES, width), jnp.float32)
            for step in order(steps, direction):
                rows = slice(step * SUBLANES, (step + 1) * SUBLANES)
                hold = keep[direction, rows, cols]
                new_re = hold * (rate_re * h_re - rate_im * h_im) + push[direction, 0, rows, cols]
                h_im = hold * (rate_re * h_im + rate_im * h_re) + push[direction, 1, rows, cols]
                h_re = new_re
                kept = kept * hold
            power_re, power_im = complex_power(rate_re, rate_im, steps)
            decay_re, decay_im = kept * power_re, kept * power_im
            for part, value in enumerate((h_re, h_im, decay_re, decay_im)):
                sub_ref[direction, part, :, cols] = value
            e_re = jnp.zeros((1, width), jnp.float32)
            e_im = jnp.zeros((1, width), jnp.float32)
            for j in order(SUBLANES, direction):
                d_re, d_im = decay_re[j : j + 1], decay_im[j : j + 1]
                e_re, e_im = (
                    d_re * e_re - d_im * e_im + h_re[j : j + 1],
                    d_re * e_im + d_im * e_re + h_im[j : j + 1],
                )
            put(direction, 0, column, e_re)
            put(direction, 1, column, e_im)


    ends_ref[...] = ends_wide[...].astype(jnp.bfloat16)
    pl.semaphore_wait(barrier, devices - 1)
    for k in range(1, count):
        copy = pltpu.make_async_remote_copy(
            src_ref=ends_ref.at[(mine + k) // count],
            dst_ref=all_ref.at[mine],
            send_sem=send_sem,
            recv_sem=recv_sem,
            device_id={"sp": lax.rem(mine + k, count)},
            device_id_type=pl.DeviceIdType.MESH,
        )
        copy.start()
    all_ref[mine] = jnp.zeros(ends_ref.shape[1:], jnp.bfloat16)

    for copy in stages[8:]:
        copy.wait()
    out_maps = (wide_out, narrow_out)
    for pack in packs:
        which, number, column, width, states = pack
        cols = slice(column, column + width)
        at = slice(number * per, (number + 1) * per)
        lanes = slice(which * half + number * LANES, which * half + (number + 1) * LANES)
        for direction in range(2):
            for part in range(2):
                rows = out_maps[which][direction, part, at].reshape(LANES, states)
                leave[direction, part, :, cols] = block_diagonal(
                    -rows if part else rows, channels, states
                )
        gates[:, lanes] = block_diagonal(
            gate_ref[which, at].astype(jnp.float32).reshape(LANES, channels), channels, channels
        )
    slots = devices * capacity
    slot = lax.broadcasted_iota(jnp.int32, (slots, own_rows), 0)
    expert = (slot // capacity) ^ (mine * n_tp + tp)
    picked = [routes[k : k + 1, :] == expert for k in range(routes.shape[0])]
    chosen = picked[0]
    for each in picked[1:]:
        chosen = jnp.logical_or(chosen, each)
    chosen = jnp.where(chosen, 1.0, 0.0)
    earlier = jnp.where(
        lax.broadcasted_iota(jnp.int32, (own_rows, own_rows), 0)
        < lax.broadcasted_iota(jnp.int32, (own_rows, own_rows), 1),
        1.0, 0.0,
    ).astype(jnp.bfloat16)
    rank = jnp.dot(chosen.astype(jnp.bfloat16), earlier, preferred_element_type=jnp.float32)
    here = rank == (slot % capacity).astype(jnp.float32)
    spot = jnp.where(here, chosen, 0.0).astype(jnp.bfloat16)
    share = route_weights[...]
    total_share = share[0:1]
    for k in range(1, share.shape[0]):
        total_share = total_share + share[k : k + 1]
    weight = jnp.zeros((slots, own_rows), jnp.float32)
    for k, each in enumerate(picked):
        weight = weight + jnp.where(
            jnp.logical_and(each, here), share[k : k + 1] / total_share, 0.0
        )
    weight = weight.T
    high = weight.astype(jnp.bfloat16)
    weights = jnp.concatenate(
        [high, (weight - high.astype(jnp.float32)).astype(jnp.bfloat16)], axis=0
    )
    sent = all_ref.at[pl.ds(0, count - 1)]
    ends = pltpu.make_async_remote_copy(
        src_ref=sent, dst_ref=sent, send_sem=send_sem, recv_sem=recv_sem,
        device_id={"sp": lax.rem(mine + 1, count)}, device_id_type=pl.DeviceIdType.MESH,
    )
    ends.wait()

    all_wide[...] = all_ref[...].astype(jnp.float32)
    shares = jnp.concatenate(
        [all_wide[b, 6:7, : 3 * n_groups] for b in range(count)], axis=0
    ).astype(jnp.bfloat16)
    for pack in packs:
        which, number, column, width, states = pack
        cols = slice(column, column + width)
        line, start = column // span, column % span
        kept = jnp.dot(
            shares, owners(pack, groups, n_groups, channels), preferred_element_type=jnp.float32
        )
        for direction in range(2):
            rate_re, rate_im = rates[direction, column]
            power_re, power_im = complex_power(rate_re, rate_im, tokens)
            c_re = jnp.zeros((1, width), jnp.float32)
            c_im = jnp.zeros((1, width), jnp.float32)
            for b in order(count, direction):
                use = b < mine if direction == 0 else b > mine
                e_re = all_wide[b, line : line + 1, start : start + width]
                e_im = all_wide[b, 3 + line : 4 + line, start : start + width]
                d_re, d_im = kept[b : b + 1] * power_re, kept[b : b + 1] * power_im
                c_re, c_im = (
                    jnp.where(use, d_re * c_re - d_im * c_im + e_re, c_re),
                    jnp.where(use, d_re * c_im + d_im * c_re + e_im, c_im),
                )
            for j in order(SUBLANES, direction):
                carry[direction, 0, j : j + 1, cols] = c_re
                carry[direction, 1, j : j + 1, cols] = c_im
                d_re = sub_ref[direction, 2, j : j + 1, cols]
                d_im = sub_ref[direction, 3, j : j + 1, cols]
                c_re, c_im = (
                    d_re * c_re - d_im * c_im + sub_ref[direction, 0, j : j + 1, cols],
                    d_re * c_im + d_im * c_re + sub_ref[direction, 1, j : j + 1, cols],
                )
    for pack in packs:
        which, number, column, width, states = pack
        cols = slice(column, column + width)
        at = slice(number * per, (number + 1) * per)
        lanes = slice(which * half + number * LANES, which * half + (number + 1) * LANES)
        local = slice(number * LANES, (number + 1) * LANES)
        read = None
        for direction in range(2):
            rate_re, rate_im = rates[direction, column]
            h_re = carry[direction, 0, :, cols]
            h_im = carry[direction, 1, :, cols]
            for step in order(steps, direction):
                rows = slice(step * SUBLANES, (step + 1) * SUBLANES)
                hold = keep[direction, rows, cols]
                new_re = hold * (rate_re * h_re - rate_im * h_im) + push[direction, 0, rows, cols]
                h_im = hold * (rate_re * h_im + rate_im * h_re) + push[direction, 1, rows, cols]
                h_re = new_re
                push[direction, 0, rows, cols] = h_re
                push[direction, 1, rows, cols] = h_im
            for part in range(2):
                term = lax.dot_general(
                    push[direction, part, :, cols].astype(jnp.bfloat16),
                    leave[direction, part, :, cols],
                    (((1,), (1,)), ((), ())),
                    preferred_element_type=jnp.float32,
                )
                read = term if read is None else read + term
        shaped = read + skip_ref[which : which + 1, local].astype(jnp.float32) * signal[
            :, lanes
        ].astype(jnp.float32)
        active = jax.nn.gelu(shaped, approximate=True)
        opened = jax.nn.sigmoid(
            jnp.dot(active.astype(jnp.bfloat16), gates[:, lanes], preferred_element_type=jnp.float32)
        )
        mixed[:, lanes] = jnp.dot(
            unweave, (active * opened).astype(jnp.bfloat16), preferred_element_type=jnp.float32
        ).astype(jnp.bfloat16)
    rows = tokens // n_tp
    swaps = []
    for k in range(1, n_tp):
        other = lax.rem(tp + k, n_tp)
        copy = pltpu.make_async_remote_copy(
            src_ref=mixed.at[pl.ds(pl.multiple_of(other * rows, rows), rows)],
            dst_ref=out_ref.at[tp],
            send_sem=swap_sem.at[0, k],
            recv_sem=swap_sem.at[1, k],
            device_id={"tp": other},
            device_id_type=pl.DeviceIdType.MESH,
        )
        copy.start()
        swaps.append(copy)
    out_ref[tp] = mixed[pl.ds(pl.multiple_of(tp * rows, rows), rows), :]
    for copy in swaps:
        copy.wait()


    parts = [
        (out_ref[k, :, which * half : (which + 1) * half], which, k)
        for which in range(2) for k in range(n_tp)
    ]
    joined = jnp.concatenate([value.astype(jnp.float32) for value, _, _ in parts], axis=1)
    scale = rms_scale(joined, joined.shape[1])
    moved = (joined * scale * mixer_gain[...]).astype(jnp.bfloat16)
    loads[0].wait()

    lead, rest = send_order(devices)
    for part in range(model // TILE):
        cols = slice(part * TILE, (part + 1) * TILE)
        value = (
            residual[:, cols].astype(jnp.float32)
            + jnp.dot(moved, out_w[:, cols], preferred_element_type=jnp.float32)
        ).astype(jnp.bfloat16)
        own[:, cols] = value.astype(jnp.float32)
        rows = jnp.dot(spot, value, preferred_element_type=jnp.float32)
        send_d[:, :, cols] = rows.reshape(devices, capacity, -1).astype(jnp.bfloat16)
        for r in lead:
            exchange(0, send_d, recv_d, r, part).start()
    for r in rest:
        exchange(0, send_d, recv_d, r).start()
    recv_d[0] = send_d[0]
    for copy in loads[1:]:
        copy.wait()
    for a, b in spans:
        whole(0, send_d, recv_d, max(a, 1), b).wait_recv()
        rows = (b - a) * capacity
        squares = jnp.zeros((rows, 1), jnp.float32)
        for start in range(0, model, TILE):
            value = recv_d[a:b, :, start : start + TILE].astype(jnp.float32).reshape(rows, -1)
            squares = squares + jnp.sum(value * value, axis=1, keepdims=True)
        scale = lax.rsqrt(squares / model + epsilon)
        for start in range(0, model, TILE):
            cols = slice(start, start + TILE)
            value = recv_d[a:b, :, cols].astype(jnp.float32).reshape(rows, -1)
            normed[:rows, cols] = (value * scale * ffn_gain[:, cols]).astype(jnp.bfloat16)

        def up(cols, rows=rows):
            value = normed[:rows, :]
            gate_val = jnp.dot(value, gate_w[:, cols], preferred_element_type=jnp.float32)
            up_val = jnp.dot(value, up_w[:, cols], preferred_element_type=jnp.float32)
            inner[:rows, cols] = (jax.nn.silu(gate_val) * up_val).astype(jnp.bfloat16)

        tiles(inner.shape[1], 256, up)

        def down(cols, a=a, b=b, rows=rows):
            value = jnp.dot(inner[:rows, :], down_w[:, cols], preferred_element_type=jnp.float32)
            send_o[a:b, :, cols] = value.reshape(b - a, capacity, -1).astype(jnp.bfloat16)

        tiles(model, 512, down)
        if a == 0:
            recv_o[0] = send_o[0]
        for r in range(max(a, 1), b):
            exchange(1, send_o, recv_o, r).start()
    for a, b in spans:
        whole(1, send_o, recv_o, max(a, 1), b).wait_recv()
        part = weights[:, a * capacity : b * capacity]

        def gather(cols, a=a, b=b, part=part):
            rows = recv_o[a:b, :, cols].astype(jnp.float32)
            rows = rows.reshape((b - a) * capacity, -1).astype(jnp.bfloat16)
            both = jnp.dot(part, rows, preferred_element_type=jnp.float32)
            own[:, cols] = own[:, cols] + (both[:own_rows] + both[own_rows:])

        tiles(model, 512, gather)
    result[...] = own[...].astype(jnp.bfloat16)
    whole(0, send_d, recv_d, 1, devices).wait_send()
    whole(1, send_o, recv_o, 1, devices).wait_send()


def local(*args):
    args = list(args)
    names = (
        "wide_inputs", "narrow_inputs", "wide_poles", "narrow_poles", "step_sizes", "forget",
        "wide_in_map", "narrow_in_map", "wide_out_map", "narrow_out_map", "skip_weight",
        "gate_mix", "residual", "mixer_gain", "out_proj", "ffn_gain", "routes", "route_weights",
        "gate_proj", "up_proj", "down_proj",
    )
    by = dict(zip(names, args))
    by["mixer_gain"] = by["mixer_gain"].reshape(1, -1)
    by["ffn_gain"] = by["ffn_gain"].reshape(1, -1)
    by["routes"] = by["routes"].T
    by["route_weights"] = by["route_weights"].T
    small = [by[n] for n in names if n not in ("gate_proj", "up_proj", "down_proj", "out_proj") and n not in ("mixer_gain", "ffn_gain", "routes", "route_weights")]
    small += [by[n] for n in ("mixer_gain", "ffn_gain", "routes", "route_weights")]
    big = [by[n] for n in ("gate_proj", "up_proj", "down_proj", "out_proj")]
    tokens, half = by["wide_inputs"].shape
    groups, channels, wide_state = by["wide_in_map"].shape[2:]
    narrow_state = by["narrow_in_map"].shape[4]
    _, total = pack_list(channels, groups, (wide_state, narrow_state))
    count, n_tp = lax.axis_size("sp"), lax.axis_size("tp")
    devices = count * n_tp
    own_rows, width = by["residual"].shape
    hidden_width = by["gate_proj"].shape[2]
    capacity = max(4 * tokens // (n_tp * devices), SUBLANES)
    span = total // 3
    chunk = max(b - a for a, b in chunks_of(devices)) * capacity
    vmem = pl.BlockSpec(memory_space=pltpu.VMEM)
    hbm = pl.BlockSpec(memory_space=pltpu.HBM)
    f32, bf16 = jnp.float32, jnp.bfloat16
    dma = pltpu.SemaphoreType.DMA
    return pl.pallas_call(
        layer_kernel,
        out_shape=jax.ShapeDtypeStruct((own_rows, width), bf16),
        in_specs=[hbm] * (len(small) + len(big)),
        out_specs=vmem,
        scratch_shapes=[pltpu.VMEM(x.shape, x.dtype) for x in small]
        + [pltpu.VMEM(x.shape[-2:], x.dtype) for x in big]
        + [
            pltpu.VMEM((tokens, 2 * half), bf16),
            pltpu.VMEM((2, 2, tokens, total), f32),
            pltpu.VMEM((2, tokens, total), f32),
            pltpu.VMEM((2, 8, span), bf16),
            pltpu.VMEM((2, 8, span), f32),
            pltpu.VMEM((2, 4, SUBLANES, total), f32),
            pltpu.VMEM((count, 8, span), bf16),
            pltpu.VMEM((count, 8, span), f32),
            pltpu.VMEM((2, 2, SUBLANES, total), f32),
            pltpu.VMEM((2, 2, LANES, total), bf16),
            pltpu.VMEM((LANES, 2 * half), bf16),
            pltpu.VMEM((tokens, 2 * half), bf16),
            pltpu.VMEM((n_tp, own_rows, 2 * half), bf16),
            pltpu.VMEM((devices, capacity, width), bf16),
            pltpu.VMEM((devices, capacity, width), bf16),
            pltpu.VMEM((devices, capacity, width), bf16),
            pltpu.VMEM((devices, capacity, width), bf16),
            pltpu.VMEM((own_rows, width), f32),
            pltpu.VMEM((chunk, width), bf16),
            pltpu.VMEM((chunk, hidden_width), bf16),
            dma((len(small),)),
            dma((4,)),
            dma,
            dma,
            dma((2, n_tp)),
            dma((2,)),
            dma((2, len(chunks_of(devices)))),
        ],
        compiler_params=pltpu.CompilerParams(
            collective_id=0, has_side_effects=True, vmem_limit_bytes=60 << 20
        ),
        name="layer",
    )(*small, *big)


def solution(mesh):
    return jax.shard_map(
        local,
        mesh=mesh,
        in_specs=(
            P("sp", "tp"),
            P("sp", "tp"),
            P(None, None, "tp", None),
            P(None, None, "tp", None),
            P(None, None, "tp"),
            P(None, None, "tp", "sp"),
            P(None, None, "tp", None, None),
            P(None, None, "tp", None, None),
            P(None, None, "tp", None, None),
            P(None, None, "tp", None, None),
            P(None, "tp"),
            P(None, "tp", None, None),
            P(("sp", "tp"), None),
            P(),
            P(),
            P(),
            P(("sp", "tp"), None),
            P(("sp", "tp"), None),
            P(("sp", "tp"), None, None),
            P(("sp", "tp"), None, None),
            P(("sp", "tp"), None, None),
        ),
        out_specs=P(("sp", "tp"), None),
        check_vma=False,
    )
```

```python
import jax
import jax.numpy as jnp
from jax import lax
from jax.experimental import pallas as pl
from jax.experimental.pallas import tpu as pltpu
from jax.sharding import PartitionSpec as P

epsilon = 1e-06
SUBLANES = 8
LANES = 128
TILE = 512
EARLY_PARTS = 2


def complex_power(re, im, exponent):
    out_re, out_im = None, None
    while exponent:
        if exponent & 1:
            if out_re is None:
                out_re, out_im = re, im
            else:
                out_re, out_im = out_re * re - out_im * im, out_re * im + out_im * re
        re, im = re * re - im * im, 2.0 * re * im
        exponent >>= 1
    return out_re, out_im


def pack_list(channels, groups, sets):
    per = LANES // channels
    packs, column = [], 0
    for which, states in enumerate(sets):
        for pack in range(groups // per):
            packs.append((which, pack, column, per * states, states))
            column += per * states
    return packs, column


def order(count, direction):
    return range(count) if direction == 0 else range(count - 1, -1, -1)


def widen(rows, copies):
    return jnp.concatenate([rows] * copies, axis=1)


def block_diagonal(rows, channels, states):
    copies = LANES // channels
    tiled = widen(rows, copies)
    row = lax.broadcasted_iota(jnp.int32, tiled.shape, 0) // channels
    column = lax.broadcasted_iota(jnp.int32, tiled.shape, 1) // states
    return jnp.where(row == column, tiled, 0.0).astype(jnp.bfloat16)


def flat_row(rows, states):
    copies = rows.shape[0]
    tiled = widen(rows, copies)
    row = lax.broadcasted_iota(jnp.int32, tiled.shape, 0)
    column = lax.broadcasted_iota(jnp.int32, tiled.shape, 1) // states
    return jnp.sum(jnp.where(row == column, tiled, 0.0), axis=0, keepdims=True)


def split3(value):
    high = value.astype(jnp.bfloat16)
    rest = value - high.astype(jnp.float32)
    mid = rest.astype(jnp.bfloat16)
    low = (rest - mid.astype(jnp.float32)).astype(jnp.bfloat16)
    return high, mid, low


def owners(pack, groups, count, channels):
    which, number, _, width, states = pack
    first = which * groups + number * (LANES // channels)
    row = lax.broadcasted_iota(jnp.int32, (3 * count, width), 0) % count
    column = first + lax.broadcasted_iota(jnp.int32, (3 * count, width), 1) // states
    return jnp.where(row == column, 1.0, 0.0).astype(jnp.bfloat16)


def flip(value, bits):
    bit = 1
    while bit <= bits:
        if bits & bit:
            value = value + bit - 2 * bit * ((value // bit) % 2)
        bit *= 2
    return value


def rms_scale(value, width):
    return lax.rsqrt(jnp.sum(value * value, axis=1, keepdims=True) / width + epsilon)


def tiles(width, tile, step):
    full = width // tile
    if full:

        @pl.loop(0, full)
        def _(j):
            step(pl.ds(pl.multiple_of(j * tile, tile), tile))

    if width % tile:
        step(slice(full * tile, width))


def chunks_of(devices):
    near, far = min(16, devices // 2), min(16, devices // 4)
    half = devices // 2
    return [(a, a + near) for a in range(0, half, near)] + [
        (a, a + far) for a in range(half, devices, far)
    ]


def send_order(devices):
    half, quarter = devices // 2, devices // 4
    first = list(range(half, half + quarter))
    near = list(range(1, half))
    last = list(range(half + quarter, devices))
    rest = []
    for i, r in enumerate(last):
        rest.append(r)
        rest += near[i * len(near) // len(last) : (i + 1) * len(near) // len(last)]
    return first, rest


def early_span(devices):
    first = devices // 2 + devices // 4
    return first, first + max(1, devices * EARLY_PARTS // 32)


N_SMALL = 17


def layer_kernel(*refs):
    small_hbm, refs = refs[:N_SMALL], refs[N_SMALL:]
    big_hbm, refs = refs[:4], refs[4:]
    result, refs = refs[0], refs[1:]
    small, refs = refs[:N_SMALL], refs[N_SMALL:]
    big, refs = refs[:4], refs[4:]
    (
        wide_u, narrow_u, wide_poles, narrow_poles, step_ref, forget_ref, wide_in, narrow_in,
        wide_out, narrow_out, skip_ref, gate_ref, residual, mixer_gain, ffn_gain, routes,
        route_weights,
    ) = small
    gate_w, up_w, down_w, out_w = big
    (
        signal, push, keep, ends_ref, ends_wide, sub_ref, all_ref, all_wide, carry, leave, gates, mixed, out_ref, send_d, recv_d,
        send_r, recv_r, send_m, recv_m, send_o, recv_o, own, normed, inner,
        small_sem, big_sem, send_sem, recv_sem, swap_sem, send_sems, recv_sems, tail_sems, early_sems,
    ) = refs
    tokens, half = wide_u.shape
    groups, channels = wide_in.shape[2:4]
    sets = (wide_in.shape[4], narrow_in.shape[4])
    packs, total = pack_list(channels, groups, sets)
    per = LANES // channels
    steps = tokens // SUBLANES
    span = ends_ref.shape[2]
    count = lax.axis_size("sp")
    n_tp = lax.axis_size("tp")
    mine = lax.axis_index("sp")
    tp = lax.axis_index("tp")
    devices, capacity, model = send_d.shape
    own_rows = residual.shape[0]
    others = [(r // n_tp, r % n_tp) for r in range(devices)]
    peers = [{"sp": flip(mine, a), "tp": flip(tp, b)} for a, b in others]
    barrier = pltpu.get_barrier_semaphore()
    for r in range(1, devices):
        pl.semaphore_signal(
            barrier, inc=1, device_id=peers[r], device_id_type=pl.DeviceIdType.MESH
        )
    stages = []
    for i in (0, 1, 5, 2, 3, 4, 6, 7, 8, 9, 10, 11, 12, 13, 14, 15, 16):
        copy = pltpu.make_async_copy(small_hbm[i], small[i], small_sem.at[i])
        copy.start()
        stages.append(copy)
    loads = []
    for i in (3, 0, 1, 2):
        source = big_hbm[i] if i == 3 else big_hbm[i].at[0]
        loads.append(pltpu.make_async_copy(source, big[i], big_sem.at[i]))

    spans = chunks_of(devices)

    def group_of(r):
        return [a <= r < b for a, b in spans].index(True)

    def whole(which, source, target, first, last):
        at = pl.ds(first, last - first)
        return pltpu.make_async_remote_copy(
            src_ref=source.at[at], dst_ref=target.at[at],
            send_sem=send_sems.at[which], recv_sem=recv_sems.at[which, group_of(first)],
            device_id=peers[1], device_id_type=pl.DeviceIdType.MESH,
        )

    def exchange(which, source, target, r, part=None):
        at = (r,) if part is None else (r, slice(None), slice(part * TILE, (part + 1) * TILE))
        return pltpu.make_async_remote_copy(
            src_ref=source.at[at], dst_ref=target.at[at],
            send_sem=send_sems.at[which],
            recv_sem=tail_sems.at[part]
            if which and part is not None
            else recv_sems.at[which, group_of(r)],
            device_id=peers[r], device_id_type=pl.DeviceIdType.MESH,
        )

    for copy in stages[:8]:
        copy.wait()
    for copy in loads:
        copy.start()

    row = lax.broadcasted_iota(jnp.int32, (tokens, tokens), 0)
    column = lax.broadcasted_iota(jnp.int32, (tokens, tokens), 1)
    weave = jnp.where(
        column == (row % SUBLANES) * steps + row // SUBLANES, 1.0, 0.0
    ).astype(jnp.bfloat16)
    unweave = jnp.where(
        row == (column % SUBLANES) * steps + column // SUBLANES, 1.0, 0.0
    ).astype(jnp.bfloat16)
    inputs = (wide_u, narrow_u)
    for which in range(2):
        signal[:, which * half : (which + 1) * half] = jnp.dot(
            weave, inputs[which][...], preferred_element_type=jnp.float32
        ).astype(jnp.bfloat16)
    held = []
    n_groups = 2 * groups
    for direction in range(2):
        rows = jnp.concatenate([forget_ref[direction, 0], forget_ref[direction, 1]], axis=0)
        pieces = jnp.concatenate(split3(jnp.exp(-rows)), axis=0)
        held.append(
            lax.dot_general(
                weave, pieces, (((1,), (1,)), ((), ())), preferred_element_type=jnp.float32
            ).astype(jnp.bfloat16)
        )
        sums = lax.dot_general(
            jnp.ones((SUBLANES, tokens), jnp.float32), rows, (((1,), (1,)), ((), ())),
            precision=lax.Precision.HIGHEST, preferred_element_type=jnp.float32,
        )
        ends_wide[direction, 6:8, :] = jnp.zeros((2, span), jnp.float32)
        ends_wide[direction, 6:7, : 3 * n_groups] = jnp.concatenate(
            [piece.astype(jnp.float32) for piece in split3(jnp.exp(-sums))], axis=1
        )[:1]

    def put(direction, part, column, value):
        done = 0
        while done < value.shape[1]:
            at = column + done
            line, start = at // span, at % span
            size = min(value.shape[1] - done, span - start)
            ends_wide[direction, 3 * part + line : 3 * part + line + 1, start : start + size] = (
                value[:, done : done + size]
            )
            done += size

    eye_row = lax.broadcasted_iota(jnp.int32, (per, groups), 0)
    eye_column = lax.broadcasted_iota(jnp.int32, (per, groups), 1)
    poles, in_maps = (wide_poles, narrow_poles), (wide_in, narrow_in)
    rates = {}
    for pack in packs:
        which, number, column, width, states = pack
        cols = slice(column, column + width)
        at = slice(number * per, (number + 1) * per)
        lanes = slice(which * half + number * LANES, which * half + (number + 1) * LANES)
        owner = owners(pack, groups, n_groups, channels)
        for direction in range(2):
            re, im = poles[which][direction, 0, at, :], poles[which][direction, 1, at, :]
            growth = jnp.exp(re)
            rate_re, rate_im = growth * jnp.cos(im), growth * jnp.sin(im)
            numer = rate_re - 1.0
            step = jnp.sum(
                jnp.where(
                    eye_column == eye_row + number * per,
                    step_ref[direction, which : which + 1, :], 0.0,
                ),
                axis=1, keepdims=True,
            )
            scale = step / (re * re + im * im)
            factor_re = ((numer * re + rate_im * im) * scale)[:, None, :]
            factor_im = ((rate_im * re - numer * im) * scale)[:, None, :]
            in_re, in_im = in_maps[which][direction, 0, at], in_maps[which][direction, 1, at]
            enter = (factor_re * in_re - factor_im * in_im, factor_re * in_im + factor_im * in_re)
            for part in range(2):
                push[direction, part, :, cols] = jnp.dot(
                    signal[:, lanes],
                    block_diagonal(enter[part].reshape(LANES, states), channels, states),
                    preferred_element_type=jnp.float32,
                )
            keep[direction, :, cols] = jnp.dot(
                held[direction], owner, preferred_element_type=jnp.float32
            )
            rate_re, rate_im = flat_row(rate_re, states), flat_row(rate_im, states)
            rates[direction, column] = (rate_re, rate_im)
            h_re = jnp.zeros((SUBLANES, width), jnp.float32)
            h_im = jnp.zeros((SUBLANES, width), jnp.float32)
            kept = jnp.ones((SUBLANES, width), jnp.float32)
            for step in order(steps, direction):
                rows = slice(step * SUBLANES, (step + 1) * SUBLANES)
                hold = keep[direction, rows, cols]
                new_re = hold * (rate_re * h_re - rate_im * h_im) + push[direction, 0, rows, cols]
                h_im = hold * (rate_re * h_im + rate_im * h_re) + push[direction, 1, rows, cols]
                h_re = new_re
                kept = kept * hold
            power_re, power_im = complex_power(rate_re, rate_im, steps)
            decay_re, decay_im = kept * power_re, kept * power_im
            for part, value in enumerate((h_re, h_im, decay_re, decay_im)):
                sub_ref[direction, part, :, cols] = value
            e_re = jnp.zeros((1, width), jnp.float32)
            e_im = jnp.zeros((1, width), jnp.float32)
            for j in order(SUBLANES, direction):
                d_re, d_im = decay_re[j : j + 1], decay_im[j : j + 1]
                e_re, e_im = (
                    d_re * e_re - d_im * e_im + h_re[j : j + 1],
                    d_re * e_im + d_im * e_re + h_im[j : j + 1],
                )
            put(direction, 0, column, e_re)
            put(direction, 1, column, e_im)


    ends_ref[...] = ends_wide[...].astype(jnp.bfloat16)
    pl.semaphore_wait(barrier, devices - 1)
    for k in range(1, count):
        copy = pltpu.make_async_remote_copy(
            src_ref=ends_ref.at[(mine + k) // count],
            dst_ref=all_ref.at[mine],
            send_sem=send_sem,
            recv_sem=recv_sem,
            device_id={"sp": lax.rem(mine + k, count)},
            device_id_type=pl.DeviceIdType.MESH,
        )
        copy.start()
    all_ref[mine] = jnp.zeros(ends_ref.shape[1:], jnp.bfloat16)

    for copy in stages[8:]:
        copy.wait()
    out_maps = (wide_out, narrow_out)
    for pack in packs:
        which, number, column, width, states = pack
        cols = slice(column, column + width)
        at = slice(number * per, (number + 1) * per)
        lanes = slice(which * half + number * LANES, which * half + (number + 1) * LANES)
        for direction in range(2):
            for part in range(2):
                rows = out_maps[which][direction, part, at].reshape(LANES, states)
                leave[direction, part, :, cols] = block_diagonal(
                    -rows if part else rows, channels, states
                )
        gates[:, lanes] = block_diagonal(
            gate_ref[which, at].astype(jnp.float32).reshape(LANES, channels), channels, channels
        )
    slots = devices * capacity
    slot = lax.broadcasted_iota(jnp.int32, (slots, own_rows), 0)
    expert = (slot // capacity) ^ (mine * n_tp + tp)
    picked = [routes[k : k + 1, :] == expert for k in range(routes.shape[0])]
    chosen = picked[0]
    for each in picked[1:]:
        chosen = jnp.logical_or(chosen, each)
    chosen = jnp.where(chosen, 1.0, 0.0)
    earlier = jnp.where(
        lax.broadcasted_iota(jnp.int32, (own_rows, own_rows), 0)
        < lax.broadcasted_iota(jnp.int32, (own_rows, own_rows), 1),
        1.0, 0.0,
    ).astype(jnp.bfloat16)
    rank = jnp.dot(chosen.astype(jnp.bfloat16), earlier, preferred_element_type=jnp.float32)
    here = rank == (slot % capacity).astype(jnp.float32)
    spot = jnp.where(here, chosen, 0.0).astype(jnp.bfloat16)
    share = route_weights[...]
    total_share = share[0:1]
    for k in range(1, share.shape[0]):
        total_share = total_share + share[k : k + 1]
    weight = jnp.zeros((slots, own_rows), jnp.float32)
    for k, each in enumerate(picked):
        weight = weight + jnp.where(
            jnp.logical_and(each, here), share[k : k + 1] / total_share, 0.0
        )
    weight = weight.T
    early_a, early_b = early_span(devices)
    early_spot = spot[early_a * capacity : early_b * capacity]

    def early_copy(which, source, target, r):
        return pltpu.make_async_remote_copy(
            src_ref=source.at[r - early_a], dst_ref=target.at[r - early_a],
            send_sem=early_sems.at[0, which], recv_sem=early_sems.at[1, which],
            device_id=peers[r], device_id_type=pl.DeviceIdType.MESH,
        )

    def early_all(which, source, target):
        return pltpu.make_async_remote_copy(
            src_ref=source, dst_ref=target,
            send_sem=early_sems.at[0, which], recv_sem=early_sems.at[1, which],
            device_id=peers[1], device_id_type=pl.DeviceIdType.MESH,
        )

    for start in range(0, model, TILE):
        rows = jnp.dot(
            early_spot, residual[:, start : start + TILE], preferred_element_type=jnp.float32
        )
        send_r[:, :, start : start + TILE] = rows.reshape(
            early_b - early_a, capacity, -1
        ).astype(jnp.bfloat16)
    high = weight.astype(jnp.bfloat16)
    weights = jnp.concatenate(
        [high, (weight - high.astype(jnp.float32)).astype(jnp.bfloat16)], axis=0
    )
    sent = all_ref.at[pl.ds(0, count - 1)]
    ends = pltpu.make_async_remote_copy(
        src_ref=sent, dst_ref=sent, send_sem=send_sem, recv_sem=recv_sem,
        device_id={"sp": lax.rem(mine + 1, count)}, device_id_type=pl.DeviceIdType.MESH,
    )
    ends.wait()
    for r in range(early_a, early_b):
        early_copy(0, send_r, recv_r, r).start()

    all_wide[...] = all_ref[...].astype(jnp.float32)
    shares = jnp.concatenate(
        [all_wide[b, 6:7, : 3 * n_groups] for b in range(count)], axis=0
    ).astype(jnp.bfloat16)
    for pack in packs:
        which, number, column, width, states = pack
        cols = slice(column, column + width)
        line, start = column // span, column % span
        kept = jnp.dot(
            shares, owners(pack, groups, n_groups, channels), preferred_element_type=jnp.float32
        )
        for direction in range(2):
            rate_re, rate_im = rates[direction, column]
            power_re, power_im = complex_power(rate_re, rate_im, tokens)
            c_re = jnp.zeros((1, width), jnp.float32)
            c_im = jnp.zeros((1, width), jnp.float32)
            for b in order(count, direction):
                use = b < mine if direction == 0 else b > mine
                e_re = all_wide[b, line : line + 1, start : start + width]
                e_im = all_wide[b, 3 + line : 4 + line, start : start + width]
                d_re, d_im = kept[b : b + 1] * power_re, kept[b : b + 1] * power_im
                c_re, c_im = (
                    jnp.where(use, d_re * c_re - d_im * c_im + e_re, c_re),
                    jnp.where(use, d_re * c_im + d_im * c_re + e_im, c_im),
                )
            for j in order(SUBLANES, direction):
                carry[direction, 0, j : j + 1, cols] = c_re
                carry[direction, 1, j : j + 1, cols] = c_im
                d_re = sub_ref[direction, 2, j : j + 1, cols]
                d_im = sub_ref[direction, 3, j : j + 1, cols]
                c_re, c_im = (
                    d_re * c_re - d_im * c_im + sub_ref[direction, 0, j : j + 1, cols],
                    d_re * c_im + d_im * c_re + sub_ref[direction, 1, j : j + 1, cols],
                )
    for pack in packs:
        which, number, column, width, states = pack
        cols = slice(column, column + width)
        at = slice(number * per, (number + 1) * per)
        lanes = slice(which * half + number * LANES, which * half + (number + 1) * LANES)
        local = slice(number * LANES, (number + 1) * LANES)
        read = None
        for direction in range(2):
            rate_re, rate_im = rates[direction, column]
            h_re = carry[direction, 0, :, cols]
            h_im = carry[direction, 1, :, cols]
            for step in order(steps, direction):
                rows = slice(step * SUBLANES, (step + 1) * SUBLANES)
                hold = keep[direction, rows, cols]
                new_re = hold * (rate_re * h_re - rate_im * h_im) + push[direction, 0, rows, cols]
                h_im = hold * (rate_re * h_im + rate_im * h_re) + push[direction, 1, rows, cols]
                h_re = new_re
                push[direction, 0, rows, cols] = h_re
                push[direction, 1, rows, cols] = h_im
            for part in range(2):
                term = lax.dot_general(
                    push[direction, part, :, cols].astype(jnp.bfloat16),
                    leave[direction, part, :, cols],
                    (((1,), (1,)), ((), ())),
                    preferred_element_type=jnp.float32,
                )
                read = term if read is None else read + term
        shaped = read + skip_ref[which : which + 1, local].astype(jnp.float32) * signal[
            :, lanes
        ].astype(jnp.float32)
        active = jax.nn.gelu(shaped, approximate=True)
        opened = jax.nn.sigmoid(
            jnp.dot(active.astype(jnp.bfloat16), gates[:, lanes], preferred_element_type=jnp.float32)
        )
        mixed[:, lanes] = jnp.dot(
            unweave, (active * opened).astype(jnp.bfloat16), preferred_element_type=jnp.float32
        ).astype(jnp.bfloat16)
    rows = tokens // n_tp
    swaps = []
    for k in range(1, n_tp):
        other = lax.rem(tp + k, n_tp)
        copy = pltpu.make_async_remote_copy(
            src_ref=mixed.at[pl.ds(pl.multiple_of(other * rows, rows), rows)],
            dst_ref=out_ref.at[tp],
            send_sem=swap_sem.at[0, k],
            recv_sem=swap_sem.at[1, k],
            device_id={"tp": other},
            device_id_type=pl.DeviceIdType.MESH,
        )
        copy.start()
        swaps.append(copy)
    out_ref[tp] = mixed[pl.ds(pl.multiple_of(tp * rows, rows), rows), :]
    for copy in swaps:
        copy.wait()


    parts = [
        (out_ref[k, :, which * half : (which + 1) * half], which, k)
        for which in range(2) for k in range(n_tp)
    ]
    joined = jnp.concatenate([value.astype(jnp.float32) for value, _, _ in parts], axis=1)
    scale = rms_scale(joined, joined.shape[1])
    moved = (joined * scale * mixer_gain[...]).astype(jnp.bfloat16)
    rows = jnp.dot(early_spot, moved, preferred_element_type=jnp.float32)
    send_m[...] = rows.reshape(early_b - early_a, capacity, -1).astype(jnp.bfloat16)
    for r in range(early_a, early_b):
        early_copy(1, send_m, recv_m, r).start()
    loads[0].wait()

    lead, rest = send_order(devices)
    for part in range(model // TILE):
        cols = slice(part * TILE, (part + 1) * TILE)
        value = (
            residual[:, cols].astype(jnp.float32)
            + jnp.dot(moved, out_w[:, cols], preferred_element_type=jnp.float32)
        ).astype(jnp.bfloat16)
        own[:, cols] = value.astype(jnp.float32)
        rows = jnp.dot(spot, value, preferred_element_type=jnp.float32)
        send_d[:, :, cols] = rows.reshape(devices, capacity, -1).astype(jnp.bfloat16)
        for r in lead:
            exchange(0, send_d, recv_d, r, part).start()
    for r in [x for x in rest if not early_a <= x < early_b]:
        exchange(0, send_d, recv_d, r).start()
    recv_d[0] = send_d[0]
    for copy in loads[1:]:
        copy.wait()
    fronts = [x for x in spans if x[0] in lead]
    near = [x for x in spans if x[0] < devices // 2]
    others_last = [x for x in spans if x not in fronts and x not in near]
    for a, b in fronts + near + others_last:
        if (a, b) in others_last and a <= early_a < b:
            for which, source, target in ((0, send_r, recv_r), (1, send_m, recv_m)):
                early_all(which, source, target).wait_recv()
            count_e = (early_b - early_a) * capacity
            arrived = recv_m[...].astype(jnp.float32).reshape(count_e, -1).astype(jnp.bfloat16)
            for start in range(0, model, TILE):
                cols = slice(start, start + TILE)
                value = recv_r[:, :, cols].astype(jnp.float32).reshape(count_e, -1) + jnp.dot(
                    arrived, out_w[:, cols], preferred_element_type=jnp.float32
                )
                recv_d[early_a:early_b, :, cols] = value.reshape(
                    early_b - early_a, capacity, -1
                ).astype(jnp.bfloat16)
        first = max(a, 1)
        if early_a <= first < early_b:
            first = early_b
        if first < b:
            whole(0, send_d, recv_d, first, b).wait_recv()
        rows = (b - a) * capacity
        squares = jnp.zeros((rows, 1), jnp.float32)
        for start in range(0, model, TILE):
            value = recv_d[a:b, :, start : start + TILE].astype(jnp.float32).reshape(rows, -1)
            squares = squares + jnp.sum(value * value, axis=1, keepdims=True)
        scale = lax.rsqrt(squares / model + epsilon)
        for start in range(0, model, TILE):
            cols = slice(start, start + TILE)
            value = recv_d[a:b, :, cols].astype(jnp.float32).reshape(rows, -1)
            normed[:rows, cols] = (value * scale * ffn_gain[:, cols]).astype(jnp.bfloat16)

        def up(cols, rows=rows):
            value = normed[:rows, :]
            gate_val = jnp.dot(value, gate_w[:, cols], preferred_element_type=jnp.float32)
            up_val = jnp.dot(value, up_w[:, cols], preferred_element_type=jnp.float32)
            inner[:rows, cols] = (jax.nn.silu(gate_val) * up_val).astype(jnp.bfloat16)

        tiles(inner.shape[1], 256, up)

        def down(cols, a=a, b=b, rows=rows):
            value = jnp.dot(inner[:rows, :], down_w[:, cols], preferred_element_type=jnp.float32)
            send_o[a:b, :, cols] = value.reshape(b - a, capacity, -1).astype(jnp.bfloat16)

        if (a, b) == spans[-1]:
            for part in range(model // TILE):
                down(slice(part * TILE, (part + 1) * TILE))
                for r in range(a, b):
                    exchange(1, send_o, recv_o, r, part).start()
        else:
            tiles(model, 512, down)
            for r in range(max(a, 1), b):
                exchange(1, send_o, recv_o, r).start()
        if a == 0:
            recv_o[0] = send_o[0]
    for a, b in spans:
        if (a, b) != spans[-1]:
            whole(1, send_o, recv_o, max(a, 1), b).wait_recv()
        part = weights[:, a * capacity : b * capacity]

        def gather(cols, a=a, b=b, part=part):
            rows = recv_o[a:b, :, cols].astype(jnp.float32)
            rows = rows.reshape((b - a) * capacity, -1).astype(jnp.bfloat16)
            both = jnp.dot(part, rows, preferred_element_type=jnp.float32)
            own[:, cols] = own[:, cols] + (both[:own_rows] + both[own_rows:])

        if (a, b) != spans[-1]:
            tiles(model, 512, gather)
            continue
        for line in range(model // TILE):
            cols = slice(line * TILE, (line + 1) * TILE)
            at = recv_o.at[pl.ds(a, b - a), :, cols]
            pltpu.make_async_remote_copy(
                src_ref=at, dst_ref=at, send_sem=send_sems.at[1], recv_sem=tail_sems.at[line],
                device_id=peers[1], device_id_type=pl.DeviceIdType.MESH,
            ).wait_recv()
            gather(cols)
    result[...] = own[...].astype(jnp.bfloat16)
    whole(0, send_d, recv_d, 1, early_a).wait_send()
    if early_b < devices:
        whole(0, send_d, recv_d, early_b, devices).wait_send()
    early_all(0, send_r, recv_r).wait_send()
    early_all(1, send_m, recv_m).wait_send()
    whole(1, send_o, recv_o, 1, devices).wait_send()


def local(*args):
    args = list(args)
    names = (
        "wide_inputs", "narrow_inputs", "wide_poles", "narrow_poles", "step_sizes", "forget",
        "wide_in_map", "narrow_in_map", "wide_out_map", "narrow_out_map", "skip_weight",
        "gate_mix", "residual", "mixer_gain", "out_proj", "ffn_gain", "routes", "route_weights",
        "gate_proj", "up_proj", "down_proj",
    )
    by = dict(zip(names, args))
    by["mixer_gain"] = by["mixer_gain"].reshape(1, -1)
    by["ffn_gain"] = by["ffn_gain"].reshape(1, -1)
    by["routes"] = by["routes"].T
    by["route_weights"] = by["route_weights"].T
    small = [by[n] for n in names if n not in ("gate_proj", "up_proj", "down_proj", "out_proj") and n not in ("mixer_gain", "ffn_gain", "routes", "route_weights")]
    small += [by[n] for n in ("mixer_gain", "ffn_gain", "routes", "route_weights")]
    big = [by[n] for n in ("gate_proj", "up_proj", "down_proj", "out_proj")]
    tokens, half = by["wide_inputs"].shape
    groups, channels, wide_state = by["wide_in_map"].shape[2:]
    narrow_state = by["narrow_in_map"].shape[4]
    _, total = pack_list(channels, groups, (wide_state, narrow_state))
    count, n_tp = lax.axis_size("sp"), lax.axis_size("tp")
    devices = count * n_tp
    own_rows, width = by["residual"].shape
    hidden_width = by["gate_proj"].shape[2]
    capacity = max(4 * tokens // (n_tp * devices), SUBLANES)
    span = total // 3
    early_rows = early_span(devices)[1] - early_span(devices)[0]
    chunk = max(b - a for a, b in chunks_of(devices)) * capacity
    vmem = pl.BlockSpec(memory_space=pltpu.VMEM)
    hbm = pl.BlockSpec(memory_space=pltpu.HBM)
    f32, bf16 = jnp.float32, jnp.bfloat16
    dma = pltpu.SemaphoreType.DMA
    return pl.pallas_call(
        layer_kernel,
        out_shape=jax.ShapeDtypeStruct((own_rows, width), bf16),
        in_specs=[hbm] * (len(small) + len(big)),
        out_specs=vmem,
        scratch_shapes=[pltpu.VMEM(x.shape, x.dtype) for x in small]
        + [pltpu.VMEM(x.shape[-2:], x.dtype) for x in big]
        + [
            pltpu.VMEM((tokens, 2 * half), bf16),
            pltpu.VMEM((2, 2, tokens, total), f32),
            pltpu.VMEM((2, tokens, total), f32),
            pltpu.VMEM((2, 8, span), bf16),
            pltpu.VMEM((2, 8, span), f32),
            pltpu.VMEM((2, 4, SUBLANES, total), f32),
            pltpu.VMEM((count, 8, span), bf16),
            pltpu.VMEM((count, 8, span), f32),
            pltpu.VMEM((2, 2, SUBLANES, total), f32),
            pltpu.VMEM((2, 2, LANES, total), bf16),
            pltpu.VMEM((LANES, 2 * half), bf16),
            pltpu.VMEM((tokens, 2 * half), bf16),
            pltpu.VMEM((n_tp, own_rows, 2 * half), bf16),
            pltpu.VMEM((devices, capacity, width), bf16),
            pltpu.VMEM((devices, capacity, width), bf16),
            pltpu.VMEM((early_rows, capacity, width), bf16),
            pltpu.VMEM((early_rows, capacity, width), bf16),
            pltpu.VMEM((early_rows, capacity, 2 * half * n_tp), bf16),
            pltpu.VMEM((early_rows, capacity, 2 * half * n_tp), bf16),
            pltpu.VMEM((devices, capacity, width), bf16),
            pltpu.VMEM((devices, capacity, width), bf16),
            pltpu.VMEM((own_rows, width), f32),
            pltpu.VMEM((chunk, width), bf16),
            pltpu.VMEM((chunk, hidden_width), bf16),
            dma((len(small),)),
            dma((4,)),
            dma,
            dma,
            dma((2, n_tp)),
            dma((2,)),
            dma((2, len(chunks_of(devices)))),
            dma((width // TILE,)),
            dma((2, 2)),
        ],
        compiler_params=pltpu.CompilerParams(
            collective_id=0, has_side_effects=True, vmem_limit_bytes=60 << 20
        ),
        name="layer",
    )(*small, *big)


def solution(mesh):
    return jax.shard_map(
        local,
        mesh=mesh,
        in_specs=(
            P("sp", "tp"),
            P("sp", "tp"),
            P(None, None, "tp", None),
            P(None, None, "tp", None),
            P(None, None, "tp"),
            P(None, None, "tp", "sp"),
            P(None, None, "tp", None, None),
            P(None, None, "tp", None, None),
            P(None, None, "tp", None, None),
            P(None, None, "tp", None, None),
            P(None, "tp"),
            P(None, "tp", None, None),
            P(("sp", "tp"), None),
            P(),
            P(),
            P(),
            P(("sp", "tp"), None),
            P(("sp", "tp"), None),
            P(("sp", "tp"), None, None),
            P(("sp", "tp"), None, None),
            P(("sp", "tp"), None, None),
        ),
        out_specs=P(("sp", "tp"), None),
        check_vma=False,
    )
```

```python
import jax
import jax.numpy as jnp
from jax import lax
from jax.experimental import pallas as pl
from jax.experimental.pallas import tpu as pltpu
from jax.sharding import PartitionSpec as P

epsilon = 1e-06
SUBLANES = 8
LANES = 128
TILE = 512
EARLY_PARTS = 2


def complex_power(re, im, exponent):
    out_re, out_im = None, None
    while exponent:
        if exponent & 1:
            if out_re is None:
                out_re, out_im = re, im
            else:
                out_re, out_im = out_re * re - out_im * im, out_re * im + out_im * re
        re, im = re * re - im * im, 2.0 * re * im
        exponent >>= 1
    return out_re, out_im


def pack_list(channels, groups, sets):
    per = LANES // channels
    packs, column = [], 0
    for which, states in enumerate(sets):
        for pack in range(groups // per):
            packs.append((which, pack, column, per * states, states))
            column += per * states
    return packs, column


def order(count, direction):
    return range(count) if direction == 0 else range(count - 1, -1, -1)


def widen(rows, copies):
    return jnp.concatenate([rows] * copies, axis=1)


def block_diagonal(rows, channels, states):
    copies = LANES // channels
    tiled = widen(rows, copies)
    row = lax.broadcasted_iota(jnp.int32, tiled.shape, 0) // channels
    column = lax.broadcasted_iota(jnp.int32, tiled.shape, 1) // states
    return jnp.where(row == column, tiled, 0.0).astype(jnp.bfloat16)


def flat_row(rows, states):
    copies = rows.shape[0]
    tiled = widen(rows, copies)
    row = lax.broadcasted_iota(jnp.int32, tiled.shape, 0)
    column = lax.broadcasted_iota(jnp.int32, tiled.shape, 1) // states
    return jnp.sum(jnp.where(row == column, tiled, 0.0), axis=0, keepdims=True)


def split3(value):
    high = value.astype(jnp.bfloat16)
    rest = value - high.astype(jnp.float32)
    mid = rest.astype(jnp.bfloat16)
    low = (rest - mid.astype(jnp.float32)).astype(jnp.bfloat16)
    return high, mid, low


def owners(pack, groups, count, channels):
    which, number, _, width, states = pack
    first = which * groups + number * (LANES // channels)
    row = lax.broadcasted_iota(jnp.int32, (3 * count, width), 0) % count
    column = first + lax.broadcasted_iota(jnp.int32, (3 * count, width), 1) // states
    return jnp.where(row == column, 1.0, 0.0).astype(jnp.bfloat16)


def flip(value, bits):
    bit = 1
    while bit <= bits:
        if bits & bit:
            value = value + bit - 2 * bit * ((value // bit) % 2)
        bit *= 2
    return value


def rms_scale(value, width):
    return lax.rsqrt(jnp.sum(value * value, axis=1, keepdims=True) / width + epsilon)


def tiles(width, tile, step):
    full = width // tile
    if full:

        @pl.loop(0, full)
        def _(j):
            step(pl.ds(pl.multiple_of(j * tile, tile), tile))

    if width % tile:
        step(slice(full * tile, width))


def chunks_of(devices):
    near, far = min(16, devices // 2), min(16, devices // 4)
    half = devices // 2
    return [(a, a + near) for a in range(0, half, near)] + [
        (a, a + far) for a in range(half, devices, far)
    ]


def send_order(devices):
    half, quarter = devices // 2, devices // 4
    first = list(range(half, half + quarter))
    near = list(range(1, half))
    last = list(range(half + quarter, devices))
    rest = []
    for i, r in enumerate(last):
        rest.append(r)
        rest += near[i * len(near) // len(last) : (i + 1) * len(near) // len(last)]
    return first, rest


def early_span(devices):
    first = devices // 2 + devices // 4
    return first, first + max(1, devices * EARLY_PARTS // 32)


N_SMALL = 17


def layer_kernel(*refs):
    small_hbm, refs = refs[:N_SMALL], refs[N_SMALL:]
    big_hbm, refs = refs[:4], refs[4:]
    result, refs = refs[0], refs[1:]
    small, refs = refs[:N_SMALL], refs[N_SMALL:]
    big, refs = refs[:4], refs[4:]
    (
        wide_u, narrow_u, wide_poles, narrow_poles, step_ref, forget_ref, wide_in, narrow_in,
        wide_out, narrow_out, skip_ref, gate_ref, residual, mixer_gain, ffn_gain, routes,
        route_weights,
    ) = small
    gate_w, up_w, down_w, out_w = big
    (
        signal, push, keep, ends_ref, ends_wide, sub_ref, all_ref, all_wide, carry, leave, gates, mixed, out_ref, send_d, recv_d,
        send_r, recv_r, send_m, recv_m, send_o, recv_o, own, normed, inner,
        small_sem, big_sem, send_sem, recv_sem, swap_sem, send_sems, recv_sems, tail_sems, early_sems,
    ) = refs
    tokens, half = wide_u.shape
    groups, channels = wide_in.shape[2:4]
    sets = (wide_in.shape[4], narrow_in.shape[4])
    packs, total = pack_list(channels, groups, sets)
    per = LANES // channels
    steps = tokens // SUBLANES
    span = ends_ref.shape[2]
    count = lax.axis_size("sp")
    n_tp = lax.axis_size("tp")
    mine = lax.axis_index("sp")
    tp = lax.axis_index("tp")
    devices, capacity, model = send_d.shape
    own_rows = residual.shape[0]
    others = [(r // n_tp, r % n_tp) for r in range(devices)]
    peers = [{"sp": flip(mine, a), "tp": flip(tp, b)} for a, b in others]
    barrier = pltpu.get_barrier_semaphore()
    for r in range(1, devices):
        pl.semaphore_signal(
            barrier, inc=1, device_id=peers[r], device_id_type=pl.DeviceIdType.MESH
        )
    stages = []
    for i in (0, 1, 5, 2, 3, 4, 6, 7, 8, 9, 10, 11, 12, 13, 14, 15, 16):
        copy = pltpu.make_async_copy(small_hbm[i], small[i], small_sem.at[i])
        copy.start()
        stages.append(copy)
    loads = []
    for i in (3, 0, 1, 2):
        source = big_hbm[i] if i == 3 else big_hbm[i].at[0]
        loads.append(pltpu.make_async_copy(source, big[i], big_sem.at[i]))

    spans = chunks_of(devices)

    def group_of(r):
        return [a <= r < b for a, b in spans].index(True)

    def whole(which, source, target, first, last):
        at = pl.ds(first, last - first)
        return pltpu.make_async_remote_copy(
            src_ref=source.at[at], dst_ref=target.at[at],
            send_sem=send_sems.at[which], recv_sem=recv_sems.at[which, group_of(first)],
            device_id=peers[1], device_id_type=pl.DeviceIdType.MESH,
        )

    def exchange(which, source, target, r, part=None):
        at = (r,) if part is None else (r, slice(None), slice(part * TILE, (part + 1) * TILE))
        return pltpu.make_async_remote_copy(
            src_ref=source.at[at], dst_ref=target.at[at],
            send_sem=send_sems.at[which],
            recv_sem=tail_sems.at[part]
            if which and part is not None
            else recv_sems.at[which, group_of(r)],
            device_id=peers[r], device_id_type=pl.DeviceIdType.MESH,
        )

    for copy in stages[:3]:
        copy.wait()

    row = lax.broadcasted_iota(jnp.int32, (tokens, tokens), 0)
    column = lax.broadcasted_iota(jnp.int32, (tokens, tokens), 1)
    weave = jnp.where(
        column == (row % SUBLANES) * steps + row // SUBLANES, 1.0, 0.0
    ).astype(jnp.bfloat16)
    unweave = jnp.where(
        row == (column % SUBLANES) * steps + column // SUBLANES, 1.0, 0.0
    ).astype(jnp.bfloat16)
    inputs = (wide_u, narrow_u)
    for which in range(2):
        signal[:, which * half : (which + 1) * half] = jnp.dot(
            weave, inputs[which][...], preferred_element_type=jnp.float32
        ).astype(jnp.bfloat16)
    held = []
    n_groups = 2 * groups
    for direction in range(2):
        rows = jnp.concatenate([forget_ref[direction, 0], forget_ref[direction, 1]], axis=0)
        pieces = jnp.concatenate(split3(jnp.exp(-rows)), axis=0)
        held.append(
            lax.dot_general(
                weave, pieces, (((1,), (1,)), ((), ())), preferred_element_type=jnp.float32
            ).astype(jnp.bfloat16)
        )
        sums = lax.dot_general(
            jnp.ones((SUBLANES, tokens), jnp.float32), rows, (((1,), (1,)), ((), ())),
            precision=lax.Precision.HIGHEST, preferred_element_type=jnp.float32,
        )
        ends_wide[direction, 6:8, :] = jnp.zeros((2, span), jnp.float32)
        ends_wide[direction, 6:7, : 3 * n_groups] = jnp.concatenate(
            [piece.astype(jnp.float32) for piece in split3(jnp.exp(-sums))], axis=1
        )[:1]

    def put(direction, part, column, value):
        done = 0
        while done < value.shape[1]:
            at = column + done
            line, start = at // span, at % span
            size = min(value.shape[1] - done, span - start)
            ends_wide[direction, 3 * part + line : 3 * part + line + 1, start : start + size] = (
                value[:, done : done + size]
            )
            done += size

    for copy in stages[3:8]:
        copy.wait()
    for copy in loads:
        copy.start()
    eye_row = lax.broadcasted_iota(jnp.int32, (per, groups), 0)
    eye_column = lax.broadcasted_iota(jnp.int32, (per, groups), 1)
    poles, in_maps = (wide_poles, narrow_poles), (wide_in, narrow_in)
    rates = {}
    for pack in packs:
        which, number, column, width, states = pack
        cols = slice(column, column + width)
        at = slice(number * per, (number + 1) * per)
        lanes = slice(which * half + number * LANES, which * half + (number + 1) * LANES)
        owner = owners(pack, groups, n_groups, channels)
        for direction in range(2):
            re, im = poles[which][direction, 0, at, :], poles[which][direction, 1, at, :]
            growth = jnp.exp(re)
            rate_re, rate_im = growth * jnp.cos(im), growth * jnp.sin(im)
            numer = rate_re - 1.0
            step = jnp.sum(
                jnp.where(
                    eye_column == eye_row + number * per,
                    step_ref[direction, which : which + 1, :], 0.0,
                ),
                axis=1, keepdims=True,
            )
            scale = step / (re * re + im * im)
            factor_re = ((numer * re + rate_im * im) * scale)[:, None, :]
            factor_im = ((rate_im * re - numer * im) * scale)[:, None, :]
            in_re, in_im = in_maps[which][direction, 0, at], in_maps[which][direction, 1, at]
            enter = (factor_re * in_re - factor_im * in_im, factor_re * in_im + factor_im * in_re)
            for part in range(2):
                push[direction, part, :, cols] = jnp.dot(
                    signal[:, lanes],
                    block_diagonal(enter[part].reshape(LANES, states), channels, states),
                    preferred_element_type=jnp.float32,
                )
            keep[direction, :, cols] = jnp.dot(
                held[direction], owner, preferred_element_type=jnp.float32
            )
            rate_re, rate_im = flat_row(rate_re, states), flat_row(rate_im, states)
            rates[direction, column] = (rate_re, rate_im)
            h_re = jnp.zeros((SUBLANES, width), jnp.float32)
            h_im = jnp.zeros((SUBLANES, width), jnp.float32)
            kept = jnp.ones((SUBLANES, width), jnp.float32)
            for step in order(steps, direction):
                rows = slice(step * SUBLANES, (step + 1) * SUBLANES)
                hold = keep[direction, rows, cols]
                new_re = hold * (rate_re * h_re - rate_im * h_im) + push[direction, 0, rows, cols]
                h_im = hold * (rate_re * h_im + rate_im * h_re) + push[direction, 1, rows, cols]
                h_re = new_re
                kept = kept * hold
            power_re, power_im = complex_power(rate_re, rate_im, steps)
            decay_re, decay_im = kept * power_re, kept * power_im
            for part, value in enumerate((h_re, h_im, decay_re, decay_im)):
                sub_ref[direction, part, :, cols] = value
            e_re = jnp.zeros((1, width), jnp.float32)
            e_im = jnp.zeros((1, width), jnp.float32)
            for j in order(SUBLANES, direction):
                d_re, d_im = decay_re[j : j + 1], decay_im[j : j + 1]
                e_re, e_im = (
                    d_re * e_re - d_im * e_im + h_re[j : j + 1],
                    d_re * e_im + d_im * e_re + h_im[j : j + 1],
                )
            put(direction, 0, column, e_re)
            put(direction, 1, column, e_im)


    ends_ref[...] = ends_wide[...].astype(jnp.bfloat16)
    pl.semaphore_wait(barrier, devices - 1)
    for k in range(1, count):
        copy = pltpu.make_async_remote_copy(
            src_ref=ends_ref.at[(mine + k) // count],
            dst_ref=all_ref.at[mine],
            send_sem=send_sem,
            recv_sem=recv_sem,
            device_id={"sp": lax.rem(mine + k, count)},
            device_id_type=pl.DeviceIdType.MESH,
        )
        copy.start()
    all_ref[mine] = jnp.zeros(ends_ref.shape[1:], jnp.bfloat16)

    for copy in stages[8:]:
        copy.wait()
    powers = {at: complex_power(*rate, tokens) for at, rate in rates.items()}
    out_maps = (wide_out, narrow_out)
    for pack in packs:
        which, number, column, width, states = pack
        cols = slice(column, column + width)
        at = slice(number * per, (number + 1) * per)
        lanes = slice(which * half + number * LANES, which * half + (number + 1) * LANES)
        for direction in range(2):
            for part in range(2):
                rows = out_maps[which][direction, part, at].reshape(LANES, states)
                leave[direction, part, :, cols] = block_diagonal(
                    -rows if part else rows, channels, states
                )
        gates[:, lanes] = block_diagonal(
            gate_ref[which, at].astype(jnp.float32).reshape(LANES, channels), channels, channels
        )
    slots = devices * capacity
    slot = lax.broadcasted_iota(jnp.int32, (slots, own_rows), 0)
    expert = (slot // capacity) ^ (mine * n_tp + tp)
    picked = [routes[k : k + 1, :] == expert for k in range(routes.shape[0])]
    chosen = picked[0]
    for each in picked[1:]:
        chosen = jnp.logical_or(chosen, each)
    chosen = jnp.where(chosen, 1.0, 0.0)
    earlier = jnp.where(
        lax.broadcasted_iota(jnp.int32, (own_rows, own_rows), 0)
        < lax.broadcasted_iota(jnp.int32, (own_rows, own_rows), 1),
        1.0, 0.0,
    ).astype(jnp.bfloat16)
    rank = jnp.dot(chosen.astype(jnp.bfloat16), earlier, preferred_element_type=jnp.float32)
    here = rank == (slot % capacity).astype(jnp.float32)
    spot = jnp.where(here, chosen, 0.0).astype(jnp.bfloat16)
    share = route_weights[...]
    total_share = share[0:1]
    for k in range(1, share.shape[0]):
        total_share = total_share + share[k : k + 1]
    weight = jnp.zeros((slots, own_rows), jnp.float32)
    for k, each in enumerate(picked):
        weight = weight + jnp.where(
            jnp.logical_and(each, here), share[k : k + 1] / total_share, 0.0
        )
    weight = weight.T
    early_a, early_b = early_span(devices)
    early_spot = spot[early_a * capacity : early_b * capacity]

    def early_copy(which, source, target, r):
        return pltpu.make_async_remote_copy(
            src_ref=source.at[r - early_a], dst_ref=target.at[r - early_a],
            send_sem=early_sems.at[0, which], recv_sem=early_sems.at[1, which],
            device_id=peers[r], device_id_type=pl.DeviceIdType.MESH,
        )

    def early_all(which, source, target):
        return pltpu.make_async_remote_copy(
            src_ref=source, dst_ref=target,
            send_sem=early_sems.at[0, which], recv_sem=early_sems.at[1, which],
            device_id=peers[1], device_id_type=pl.DeviceIdType.MESH,
        )

    for start in range(0, model, TILE):
        rows = jnp.dot(
            early_spot, residual[:, start : start + TILE], preferred_element_type=jnp.float32
        )
        send_r[:, :, start : start + TILE] = rows.reshape(
            early_b - early_a, capacity, -1
        ).astype(jnp.bfloat16)
    high = weight.astype(jnp.bfloat16)
    weights = jnp.concatenate(
        [high, (weight - high.astype(jnp.float32)).astype(jnp.bfloat16)], axis=0
    )
    sent = all_ref.at[pl.ds(0, count - 1)]
    ends = pltpu.make_async_remote_copy(
        src_ref=sent, dst_ref=sent, send_sem=send_sem, recv_sem=recv_sem,
        device_id={"sp": lax.rem(mine + 1, count)}, device_id_type=pl.DeviceIdType.MESH,
    )
    ends.wait()
    for r in range(early_a, early_b):
        early_copy(0, send_r, recv_r, r).start()

    all_wide[...] = all_ref[...].astype(jnp.float32)
    shares = jnp.concatenate(
        [all_wide[b, 6:7, : 3 * n_groups] for b in range(count)], axis=0
    ).astype(jnp.bfloat16)
    for pack in packs:
        which, number, column, width, states = pack
        cols = slice(column, column + width)
        line, start = column // span, column % span
        kept = jnp.dot(
            shares, owners(pack, groups, n_groups, channels), preferred_element_type=jnp.float32
        )
        for direction in range(2):
            rate_re, rate_im = rates[direction, column]
            power_re, power_im = powers[direction, column]
            c_re = jnp.zeros((1, width), jnp.float32)
            c_im = jnp.zeros((1, width), jnp.float32)
            for b in order(count, direction):
                use = b < mine if direction == 0 else b > mine
                e_re = all_wide[b, line : line + 1, start : start + width]
                e_im = all_wide[b, 3 + line : 4 + line, start : start + width]
                d_re, d_im = kept[b : b + 1] * power_re, kept[b : b + 1] * power_im
                c_re, c_im = (
                    jnp.where(use, d_re * c_re - d_im * c_im + e_re, c_re),
                    jnp.where(use, d_re * c_im + d_im * c_re + e_im, c_im),
                )
            for j in order(SUBLANES, direction):
                carry[direction, 0, j : j + 1, cols] = c_re
                carry[direction, 1, j : j + 1, cols] = c_im
                d_re = sub_ref[direction, 2, j : j + 1, cols]
                d_im = sub_ref[direction, 3, j : j + 1, cols]
                c_re, c_im = (
                    d_re * c_re - d_im * c_im + sub_ref[direction, 0, j : j + 1, cols],
                    d_re * c_im + d_im * c_re + sub_ref[direction, 1, j : j + 1, cols],
                )
    for pack in packs:
        which, number, column, width, states = pack
        cols = slice(column, column + width)
        at = slice(number * per, (number + 1) * per)
        lanes = slice(which * half + number * LANES, which * half + (number + 1) * LANES)
        local = slice(number * LANES, (number + 1) * LANES)
        read = None
        for direction in range(2):
            rate_re, rate_im = rates[direction, column]
            h_re = carry[direction, 0, :, cols]
            h_im = carry[direction, 1, :, cols]
            for step in order(steps, direction):
                rows = slice(step * SUBLANES, (step + 1) * SUBLANES)
                hold = keep[direction, rows, cols]
                new_re = hold * (rate_re * h_re - rate_im * h_im) + push[direction, 0, rows, cols]
                h_im = hold * (rate_re * h_im + rate_im * h_re) + push[direction, 1, rows, cols]
                h_re = new_re
                push[direction, 0, rows, cols] = h_re
                push[direction, 1, rows, cols] = h_im
            for part in range(2):
                term = lax.dot_general(
                    push[direction, part, :, cols].astype(jnp.bfloat16),
                    leave[direction, part, :, cols],
                    (((1,), (1,)), ((), ())),
                    preferred_element_type=jnp.float32,
                )
                read = term if read is None else read + term
        shaped = read + skip_ref[which : which + 1, local].astype(jnp.float32) * signal[
            :, lanes
        ].astype(jnp.float32)
        active = jax.nn.gelu(shaped, approximate=True)
        opened = jax.nn.sigmoid(
            jnp.dot(active.astype(jnp.bfloat16), gates[:, lanes], preferred_element_type=jnp.float32)
        )
        mixed[:, lanes] = jnp.dot(
            unweave, (active * opened).astype(jnp.bfloat16), preferred_element_type=jnp.float32
        ).astype(jnp.bfloat16)
    rows = tokens // n_tp
    swaps = []
    for k in range(1, n_tp):
        other = lax.rem(tp + k, n_tp)
        copy = pltpu.make_async_remote_copy(
            src_ref=mixed.at[pl.ds(pl.multiple_of(other * rows, rows), rows)],
            dst_ref=out_ref.at[tp],
            send_sem=swap_sem.at[0, k],
            recv_sem=swap_sem.at[1, k],
            device_id={"tp": other},
            device_id_type=pl.DeviceIdType.MESH,
        )
        copy.start()
        swaps.append(copy)
    out_ref[tp] = mixed[pl.ds(pl.multiple_of(tp * rows, rows), rows), :]
    for copy in swaps:
        copy.wait()


    parts = [
        (out_ref[k, :, which * half : (which + 1) * half], which, k)
        for which in range(2) for k in range(n_tp)
    ]
    joined = jnp.concatenate([value.astype(jnp.float32) for value, _, _ in parts], axis=1)
    scale = rms_scale(joined, joined.shape[1])
    moved = (joined * scale * mixer_gain[...]).astype(jnp.bfloat16)
    rows = jnp.dot(early_spot, moved, preferred_element_type=jnp.float32)
    send_m[...] = rows.reshape(early_b - early_a, capacity, -1).astype(jnp.bfloat16)
    for r in range(early_a, early_b):
        early_copy(1, send_m, recv_m, r).start()
    loads[0].wait()

    lead, rest = send_order(devices)
    for part in range(model // TILE):
        cols = slice(part * TILE, (part + 1) * TILE)
        value = (
            residual[:, cols].astype(jnp.float32)
            + jnp.dot(moved, out_w[:, cols], preferred_element_type=jnp.float32)
        ).astype(jnp.bfloat16)
        own[:, cols] = value.astype(jnp.float32)
        rows = jnp.dot(spot, value, preferred_element_type=jnp.float32)
        send_d[:, :, cols] = rows.reshape(devices, capacity, -1).astype(jnp.bfloat16)
        for r in lead:
            exchange(0, send_d, recv_d, r, part).start()
    for r in [x for x in rest if not early_a <= x < early_b]:
        exchange(0, send_d, recv_d, r).start()
    recv_d[0] = send_d[0]
    for copy in loads[1:]:
        copy.wait()
    fronts = [x for x in spans if x[0] in lead]
    near = [x for x in spans if x[0] < devices // 2]
    others_last = [x for x in spans if x not in fronts and x not in near]
    for a, b in fronts + near + others_last:
        if (a, b) in others_last and a <= early_a < b:
            for which, source, target in ((0, send_r, recv_r), (1, send_m, recv_m)):
                early_all(which, source, target).wait_recv()
            count_e = (early_b - early_a) * capacity
            arrived = recv_m[...].astype(jnp.float32).reshape(count_e, -1).astype(jnp.bfloat16)
            for start in range(0, model, TILE):
                cols = slice(start, start + TILE)
                value = recv_r[:, :, cols].astype(jnp.float32).reshape(count_e, -1) + jnp.dot(
                    arrived, out_w[:, cols], preferred_element_type=jnp.float32
                )
                recv_d[early_a:early_b, :, cols] = value.reshape(
                    early_b - early_a, capacity, -1
                ).astype(jnp.bfloat16)
        first = max(a, 1)
        if early_a <= first < early_b:
            first = early_b
        if first < b:
            whole(0, send_d, recv_d, first, b).wait_recv()
        rows = (b - a) * capacity
        squares = jnp.zeros((rows, 1), jnp.float32)
        for start in range(0, model, TILE):
            value = recv_d[a:b, :, start : start + TILE].astype(jnp.float32).reshape(rows, -1)
            squares = squares + jnp.sum(value * value, axis=1, keepdims=True)
        scale = lax.rsqrt(squares / model + epsilon)
        for start in range(0, model, TILE):
            cols = slice(start, start + TILE)
            value = recv_d[a:b, :, cols].astype(jnp.float32).reshape(rows, -1)
            normed[:rows, cols] = (value * scale * ffn_gain[:, cols]).astype(jnp.bfloat16)

        def up(cols, rows=rows):
            value = normed[:rows, :]
            gate_val = jnp.dot(value, gate_w[:, cols], preferred_element_type=jnp.float32)
            up_val = jnp.dot(value, up_w[:, cols], preferred_element_type=jnp.float32)
            inner[:rows, cols] = (jax.nn.silu(gate_val) * up_val).astype(jnp.bfloat16)

        tiles(inner.shape[1], 256, up)

        def down(cols, a=a, b=b, rows=rows):
            value = jnp.dot(inner[:rows, :], down_w[:, cols], preferred_element_type=jnp.float32)
            send_o[a:b, :, cols] = value.reshape(b - a, capacity, -1).astype(jnp.bfloat16)

        if (a, b) == spans[-1]:
            for part in range(model // TILE):
                down(slice(part * TILE, (part + 1) * TILE))
                for r in range(a, b):
                    exchange(1, send_o, recv_o, r, part).start()
        else:
            tiles(model, 512, down)
            for r in range(max(a, 1), b):
                exchange(1, send_o, recv_o, r).start()
        if a == 0:
            recv_o[0] = send_o[0]
    for a, b in spans:
        if (a, b) != spans[-1]:
            whole(1, send_o, recv_o, max(a, 1), b).wait_recv()
        part = weights[:, a * capacity : b * capacity]

        def gather(cols, a=a, b=b, part=part):
            rows = recv_o[a:b, :, cols].astype(jnp.float32)
            rows = rows.reshape((b - a) * capacity, -1).astype(jnp.bfloat16)
            both = jnp.dot(part, rows, preferred_element_type=jnp.float32)
            own[:, cols] = own[:, cols] + (both[:own_rows] + both[own_rows:])

        if (a, b) != spans[-1]:
            tiles(model, 512, gather)
            continue
        for line in range(model // TILE):
            cols = slice(line * TILE, (line + 1) * TILE)
            at = recv_o.at[pl.ds(a, b - a), :, cols]
            pltpu.make_async_remote_copy(
                src_ref=at, dst_ref=at, send_sem=send_sems.at[1], recv_sem=tail_sems.at[line],
                device_id=peers[1], device_id_type=pl.DeviceIdType.MESH,
            ).wait_recv()
            gather(cols)
    result[...] = own[...].astype(jnp.bfloat16)
    whole(0, send_d, recv_d, 1, early_a).wait_send()
    if early_b < devices:
        whole(0, send_d, recv_d, early_b, devices).wait_send()
    early_all(0, send_r, recv_r).wait_send()
    early_all(1, send_m, recv_m).wait_send()
    whole(1, send_o, recv_o, 1, devices).wait_send()


def local(*args):
    args = list(args)
    names = (
        "wide_inputs", "narrow_inputs", "wide_poles", "narrow_poles", "step_sizes", "forget",
        "wide_in_map", "narrow_in_map", "wide_out_map", "narrow_out_map", "skip_weight",
        "gate_mix", "residual", "mixer_gain", "out_proj", "ffn_gain", "routes", "route_weights",
        "gate_proj", "up_proj", "down_proj",
    )
    by = dict(zip(names, args))
    by["mixer_gain"] = by["mixer_gain"].reshape(1, -1)
    by["ffn_gain"] = by["ffn_gain"].reshape(1, -1)
    by["routes"] = by["routes"].T
    by["route_weights"] = by["route_weights"].T
    small = [by[n] for n in names if n not in ("gate_proj", "up_proj", "down_proj", "out_proj") and n not in ("mixer_gain", "ffn_gain", "routes", "route_weights")]
    small += [by[n] for n in ("mixer_gain", "ffn_gain", "routes", "route_weights")]
    big = [by[n] for n in ("gate_proj", "up_proj", "down_proj", "out_proj")]
    tokens, half = by["wide_inputs"].shape
    groups, channels, wide_state = by["wide_in_map"].shape[2:]
    narrow_state = by["narrow_in_map"].shape[4]
    _, total = pack_list(channels, groups, (wide_state, narrow_state))
    count, n_tp = lax.axis_size("sp"), lax.axis_size("tp")
    devices = count * n_tp
    own_rows, width = by["residual"].shape
    hidden_width = by["gate_proj"].shape[2]
    capacity = max(4 * tokens // (n_tp * devices), SUBLANES)
    span = total // 3
    early_rows = early_span(devices)[1] - early_span(devices)[0]
    chunk = max(b - a for a, b in chunks_of(devices)) * capacity
    vmem = pl.BlockSpec(memory_space=pltpu.VMEM)
    hbm = pl.BlockSpec(memory_space=pltpu.HBM)
    f32, bf16 = jnp.float32, jnp.bfloat16
    dma = pltpu.SemaphoreType.DMA
    return pl.pallas_call(
        layer_kernel,
        out_shape=jax.ShapeDtypeStruct((own_rows, width), bf16),
        in_specs=[hbm] * (len(small) + len(big)),
        out_specs=vmem,
        scratch_shapes=[pltpu.VMEM(x.shape, x.dtype) for x in small]
        + [pltpu.VMEM(x.shape[-2:], x.dtype) for x in big]
        + [
            pltpu.VMEM((tokens, 2 * half), bf16),
            pltpu.VMEM((2, 2, tokens, total), f32),
            pltpu.VMEM((2, tokens, total), f32),
            pltpu.VMEM((2, 8, span), bf16),
            pltpu.VMEM((2, 8, span), f32),
            pltpu.VMEM((2, 4, SUBLANES, total), f32),
            pltpu.VMEM((count, 8, span), bf16),
            pltpu.VMEM((count, 8, span), f32),
            pltpu.VMEM((2, 2, SUBLANES, total), f32),
            pltpu.VMEM((2, 2, LANES, total), bf16),
            pltpu.VMEM((LANES, 2 * half), bf16),
            pltpu.VMEM((tokens, 2 * half), bf16),
            pltpu.VMEM((n_tp, own_rows, 2 * half), bf16),
            pltpu.VMEM((devices, capacity, width), bf16),
            pltpu.VMEM((devices, capacity, width), bf16),
            pltpu.VMEM((early_rows, capacity, width), bf16),
            pltpu.VMEM((early_rows, capacity, width), bf16),
            pltpu.VMEM((early_rows, capacity, 2 * half * n_tp), bf16),
            pltpu.VMEM((early_rows, capacity, 2 * half * n_tp), bf16),
            pltpu.VMEM((devices, capacity, width), bf16),
            pltpu.VMEM((devices, capacity, width), bf16),
            pltpu.VMEM((own_rows, width), f32),
            pltpu.VMEM((chunk, width), bf16),
            pltpu.VMEM((chunk, hidden_width), bf16),
            dma((len(small),)),
            dma((4,)),
            dma,
            dma,
            dma((2, n_tp)),
            dma((2,)),
            dma((2, len(chunks_of(devices)))),
            dma((width // TILE,)),
            dma((2, 2)),
        ],
        compiler_params=pltpu.CompilerParams(
            collective_id=0, has_side_effects=True, vmem_limit_bytes=60 << 20
        ),
        name="layer",
    )(*small, *big)


def solution(mesh):
    return jax.shard_map(
        local,
        mesh=mesh,
        in_specs=(
            P("sp", "tp"),
            P("sp", "tp"),
            P(None, None, "tp", None),
            P(None, None, "tp", None),
            P(None, None, "tp"),
            P(None, None, "tp", "sp"),
            P(None, None, "tp", None, None),
            P(None, None, "tp", None, None),
            P(None, None, "tp", None, None),
            P(None, None, "tp", None, None),
            P(None, "tp"),
            P(None, "tp", None, None),
            P(("sp", "tp"), None),
            P(),
            P(),
            P(),
            P(("sp", "tp"), None),
            P(("sp", "tp"), None),
            P(("sp", "tp"), None, None),
            P(("sp", "tp"), None, None),
            P(("sp", "tp"), None, None),
        ),
        out_specs=P(("sp", "tp"), None),
        check_vma=False,
    )
```
